32 devices in a mesh: fs: 8 (over z, x), tp: 4 (over y, core).
Axes of the slice: x: 2, y: 2, z: 4, core: 2. Of those that a mesh axis runs over, the one named last changes fastest.
Arguments:
- late_input: bfloat16 [4096, 2048], P(('fs', 'tp')), may hold values from -6 to 6
- norm_gain: bfloat16 [2048], replicated, may hold values from 0.099609375 to 1.8984375
- gate_weight: bfloat16 [2048, 2816], P('fs', 'tp'), may hold values from -0.125 to 0.125
- up_weight: bfloat16 [2048, 2816], P('fs', 'tp'), may hold values from -0.125 to 0.125
- down_weight: bfloat16 [2048, 2816], P('fs', 'tp'), may hold values from -0.109375 to 0.109375
- early_input: bfloat16 [4096, 2048], P(('fs', 'tp')), may hold values from -6 to 6
- cotangent: bfloat16 [4096, 2048], P(('fs', 'tp')), may hold values from -6 to 6
- gate_sum: float32 [2048, 2816], P('fs', 'tp'), may hold values from -192 to 192
- up_sum: float32 [2048, 2816], P('fs', 'tp'), may hold values from -192 to 192
- down_sum: float32 [2048, 2816], P('fs', 'tp'), may hold values from -192 to 192
- gain_sum: float32 [2048], replicated, may hold values from -192 to 192
Outputs:
- late_out: bfloat16 [4096, 2048], P(('fs', 'tp'))
- early_grad: bfloat16 [4096, 2048], P(('fs', 'tp'))
- gate_sum_out: float32 [2048, 2816], P('fs', 'tp')
- up_sum_out: float32 [2048, 2816], P('fs', 'tp')
- down_sum_out: float32 [2048, 2816], P('fs', 'tp')
- gain_sum_out: float32 [2048], replicated
The draws below stay inside these ranges and needn't reach their ends.
All inputs are finite; a program needn't handle non-finite values.
Results may differ from the reference program's by a relative error of at most 0.008.
Values may be sent and summed in bfloat16 or wider, within the bound.
A program may use at most 128 MiB of HBM per device.

```python
import jax
import jax.numpy as jnp
from jax import lax

D = 2048
FF = 2816
TOKENS = 4096
N_TP = 4


def with_spikes(drawn, stream_key, source, target, blocks, factor):
    owner, partner = [(jnp.arange(drawn.shape[axis_at]) // (drawn.shape[axis_at] // blocks)).reshape([-1 if axis == axis_at else 1 for axis in range(drawn.ndim)]) for axis_at in (source, target)]
    chosen = jax.random.permutation(stream_key, blocks)[partner]
    strong = (owner == chosen) | (owner == (partner + blocks // 2) % blocks)
    return jnp.where(strong, factor * drawn, drawn)


def block_levels(rng, extent, pieces, least, high):
    level = 1.0
    for axis_at, shards_of in pieces:
        draws = jax.random.uniform(jax.random.fold_in(jax.random.fold_in(rng, 6), axis_at), (shards_of,), jnp.float32, least / len(pieces), high / len(pieces))
        level = level * jnp.repeat(jnp.exp(draws), extent[axis_at] // shards_of).reshape((-1,) + (1,) * (len(extent) - 1 - axis_at))
    return level


def scatter_about(stream_key, shape, deviation, most, split=(), dtype=jnp.bfloat16):
    level = block_levels(stream_key, shape, split, -0.22, 0.18) if split else 1.0
    result = jax.random.normal(stream_key, shape, jnp.float32) * deviation * level
    return jnp.minimum(jnp.maximum(result, -most), most).astype(dtype)


def bell_draw_with(key, extent, deviation, limit, shards, heavy, dtype=jnp.bfloat16):
    entries = deviation * jax.random.normal(key, extent, jnp.float32)
    if shards:
        entries = entries * block_levels(key, extent, shards, -0.22, 0.18)
    return jnp.clip(with_spikes(entries, jax.random.fold_in(key, 3), *heavy), -limit, limit).astype(dtype)


def setup_inputs(seed: int = 0) -> dict:
    keys = jax.random.split(jax.random.key(seed), 12)
    return {
        "late_input": scatter_about(keys[0], (TOKENS, D), 1.0, 6.0, ((0, 32),)),
        "norm_gain": jnp.clip(1.0 + 0.18 * jax.random.normal(keys[1], (D,), jnp.float32), 0.099609375, 1.8984375).astype(jnp.bfloat16),
        "gate_weight": scatter_about(keys[2], (D, FF), D ** -0.5, 0.125, ((0, 8), (1, 4))),
        "up_weight": scatter_about(keys[3], (D, FF), D ** -0.5, 0.125, ((0, 8), (1, 4))),
        "down_weight": scatter_about(keys[4], (D, FF), FF ** -0.5, 0.109375, ((0, 8), (1, 4))),
        "early_input": scatter_about(keys[5], (TOKENS, D), 1.0, 6.0, ((0, 32),)),
        "cotangent": bell_draw_with(keys[6], (TOKENS, D), 1.0, 6.0, ((0, 32),), (0, 1, 32, 2.75)),
        "gate_sum": scatter_about(keys[7], (D, FF), 32.0, 192.0, ((0, 8), (1, 4)), jnp.float32),
        "up_sum": scatter_about(keys[8], (D, FF), 32.0, 192.0, ((0, 8), (1, 4)), jnp.float32),
        "down_sum": scatter_about(keys[9], (D, FF), 32.0, 192.0, ((0, 8), (1, 4)), jnp.float32),
        "gain_sum": scatter_about(keys[10], (D,), 32.0, 192.0, (), jnp.float32),
    }


epsilon = 1e-05

def normalize(source, gain_f):
    values = source.astype(jnp.float32)
    scale = lax.rsqrt(lax.optimization_barrier(jnp.mean(values * values, axis=-1, keepdims=True)) + epsilon)
    return ((values * scale * gain_f).astype(jnp.bfloat16), scale, values)

def blocked(pairs):
    width = FF // N_TP
    total = None
    for block in range(N_TP):
        partial_value = None
        for left, right in pairs:
            term = jnp.dot(left[:, block * width:(block + 1) * width], right[:, block * width:(block + 1) * width].T, preferred_element_type=jnp.float32)
            partial_value = term if partial_value is None else partial_value + term
        rounded = lax.optimization_barrier(partial_value.astype(jnp.bfloat16)).astype(jnp.float32)
        total = rounded if total is None else total + rounded
    return total

def reference(late_input, norm_gain, gate_weight, up_weight, down_weight, early_input, cotangent, gate_sum, up_sum, down_sum, gain_sum):
    gain_f = norm_gain.astype(jnp.float32)
    normed, scale, values = normalize(late_input, gain_f)
    gate = jnp.dot(normed, gate_weight, preferred_element_type=jnp.float32)
    upper = jnp.dot(normed, up_weight, preferred_element_type=jnp.float32)
    hidden = (jax.nn.silu(gate) * upper).astype(jnp.bfloat16)
    mixed = blocked([(hidden, down_weight)])
    late_out = (values + 0.5 * mixed).astype(jnp.bfloat16)
    normed_e, scale_e, values_e = normalize(early_input, gain_f)
    gate_e = jnp.dot(normed_e, gate_weight, preferred_element_type=jnp.float32)
    upper_e = jnp.dot(normed_e, up_weight, preferred_element_type=jnp.float32)
    sigma_e = jax.nn.sigmoid(gate_e)
    hidden_e = (gate_e * sigma_e * upper_e).astype(jnp.bfloat16)
    d_hidden = 0.5 * jnp.dot(cotangent, down_weight, preferred_element_type=jnp.float32)
    d_gate = (d_hidden * upper_e * sigma_e * (1.0 + gate_e * (1.0 - sigma_e))).astype(jnp.bfloat16)
    d_up = (d_hidden * gate_e * sigma_e).astype(jnp.bfloat16)
    d_normed = blocked([(d_gate, gate_weight), (d_up, up_weight)])
    scaled_grad = d_normed * gain_f
    early_grad = (cotangent.astype(jnp.float32) + scale_e * scaled_grad - values_e * scale_e ** 3 * lax.optimization_barrier(jnp.mean(values_e * scaled_grad, axis=-1, keepdims=True))).astype(jnp.bfloat16)
    gain_sum_out = gain_sum + lax.optimization_barrier(jnp.sum(d_normed * values_e * scale_e, axis=0))
    gate_sum_out = gate_sum + jnp.dot(normed_e.T, d_gate, preferred_element_type=jnp.float32)
    up_sum_out = up_sum + jnp.dot(normed_e.T, d_up, preferred_element_type=jnp.float32)
    down_sum_out = down_sum + 0.5 * jnp.dot(cotangent.T, hidden_e, preferred_element_type=jnp.float32)
    return (late_out, early_grad, gate_sum_out, up_sum_out, down_sum_out, gain_sum_out)
```

```python
import functools

import jax
import jax.numpy as jnp
from jax import lax
from jax.experimental import pallas as pl
from jax.experimental.pallas import tpu as pltpu
from jax.sharding import PartitionSpec as P

epsilon = 1e-05
MESH = pl.DeviceIdType.MESH
VMEM_LIMIT = 60 * 1024 * 1024


def ring_place(index, n):
    odd = lax.rem(index, 2)
    half = index // 2
    return (1 - odd) * half + odd * (n - 1 - half)


def ring_index(place, n):
    back = place // (n // 2)
    return (1 - back) * (2 * place) + back * (2 * (n - 1 - place) + 1)


def neighbours(n):
    place = ring_place(lax.axis_index("fs"), n)
    right = ring_index(lax.rem(place + 1, n), n)
    left = ring_index(lax.rem(place + n - 1, n), n)
    return place, right, left


def greet(n_tp, right, left):
    me_tp = lax.axis_index("tp")
    barrier = pltpu.get_barrier_semaphore()
    for target in (right, left):
        pl.semaphore_signal(barrier, inc=1, device_id=(target, me_tp), device_id_type=MESH)
    for away in range(1, n_tp):
        peer = lax.rem(me_tp + away, n_tp)
        pl.semaphore_signal(
            barrier, inc=1, device_id=(lax.axis_index("fs"), peer), device_id_type=MESH
        )
    pl.semaphore_wait(barrier, 2 + n_tp - 1)


def gather_kernel(n, n_tp, *refs):
    gu_ref, dn_ref, late_ref, early_ref, cot_ref = refs[:5]
    gu_all, dn_all, late_all, early_all, cot_all = refs[5:10]
    send_sem, recv_sem, tp_send, tp_recv, own_sem = refs[10:]
    me_fs, me_tp = lax.axis_index("fs"), lax.axis_index("tp")
    place, right, left = neighbours(n)
    greet(n_tp, right, left)
    rows = gu_ref.shape[0]
    half = rows // 2
    tokens = late_ref.shape[0]
    pairs = ((gu_ref, gu_all), (dn_ref, dn_all))

    def window(owner, way):
        return pl.ds(pl.multiple_of(owner * rows + way * half, half), half)

    def piece(step, c, way, first):
        block, whole = pairs[c]
        if way == 0:
            owner = ring_index(lax.rem(place - step + n, n), n)
            target = right
        else:
            owner = ring_index(lax.rem(place + step, n), n)
            target = left
        spot = whole.at[window(owner, way)]
        source = block.at[pl.ds(way * half, half)] if first else spot
        return pltpu.make_async_remote_copy(
            src_ref=source,
            dst_ref=spot,
            send_sem=send_sem.at[step, c, way],
            recv_sem=recv_sem.at[step, c, way],
            device_id=(target, me_tp),
            device_id_type=MESH,
        )

    for c in range(2):
        for way in range(2):
            piece(0, c, way, True).start()

    token_pairs = ((early_ref, early_all), (cot_ref, cot_all), (late_ref, late_all))
    token_copies = []
    for a, (block, whole) in enumerate(token_pairs):
        for away in range(1, n_tp):
            peer = lax.rem(me_tp + away, n_tp)
            copy = pltpu.make_async_remote_copy(
                src_ref=block,
                dst_ref=whole.at[pl.ds(pl.multiple_of(me_tp * tokens, tokens), tokens)],
                send_sem=tp_send.at[a, away - 1],
                recv_sem=tp_recv.at[a, away - 1],
                device_id=(me_fs, peer),
                device_id_type=MESH,
            )
            copy.start()
            token_copies.append(copy)
    own = []
    for a, (block, whole) in enumerate(token_pairs):
        own.append(
            pltpu.make_async_copy(
                block,
                whole.at[pl.ds(pl.multiple_of(me_tp * tokens, tokens), tokens)],
                own_sem.at[a],
            )
        )
    for c, (block, whole) in enumerate(pairs):
        own.append(
            pltpu.make_async_copy(
                block,
                whole.at[pl.ds(pl.multiple_of(me_fs * rows, rows), rows)],
                own_sem.at[3 + c],
            )
        )
    for copy in own:
        copy.start()

    def body(step, carry):
        for c in range(2):
            for way in range(2):
                piece(step - 1, c, way, False).wait_recv()
                piece(step, c, way, False).start()
        return carry

    lax.fori_loop(1, n - 1, body, 0)
    for c in range(2):
        for way in range(2):
            piece(n - 2, c, way, False).wait_recv()
            piece(0, c, way, True).wait_send()

    def drain(step, carry):
        for c in range(2):
            for way in range(2):
                piece(step, c, way, False).wait_send()
        return carry

    lax.fori_loop(1, n - 1, drain, 0)
    for copy in own:
        copy.wait()
    for copy in token_copies:
        copy.wait()


def gather(n, n_tp, gu, dn, late, early, cot):
    rows, width2 = gu.shape
    tokens, depth = late.shape
    vmem = pl.BlockSpec(memory_space=pltpu.VMEM)
    hbm = pl.BlockSpec(memory_space=pl.ANY)
    bf16 = jnp.bfloat16
    return pl.pallas_call(
        functools.partial(gather_kernel, n, n_tp),
        out_shape=[
            jax.ShapeDtypeStruct((n * rows, width2), bf16),
            jax.ShapeDtypeStruct((n * rows, dn.shape[1]), bf16),
        ]
        + [jax.ShapeDtypeStruct((n_tp * tokens, depth), bf16)] * 3,
        in_specs=[vmem] * 5,
        out_specs=[hbm] * 5,
        scratch_shapes=[
            pltpu.SemaphoreType.DMA((n - 1, 2, 2)),
            pltpu.SemaphoreType.DMA((n - 1, 2, 2)),
            pltpu.SemaphoreType.DMA((3, n_tp - 1)),
            pltpu.SemaphoreType.DMA((3, n_tp - 1)),
            pltpu.SemaphoreType.DMA((5,)),
        ],
        compiler_params=pltpu.CompilerParams(
            collective_id=0, has_side_effects=True, vmem_limit_bytes=VMEM_LIMIT
        ),
    )(gu, dn, late, early, cot)


def reduce_kernel(n, n_tp, *refs):
    gu_ref, dn_ref, mix_ref, dnorm_ref, gain_ref = refs[:5]
    gu_out, dn_out, mix_out, dnorm_out, gain_out = refs[5:10]
    (gu_slots, dn_slots, gain_slots, gain_tp) = refs[10:14]
    send_sem, recv_sem, gain_send, gain_recv, tp_send, tp_recv, last_send, last_recv = refs[14:]
    me_fs, me_tp = lax.axis_index("fs"), lax.axis_index("tp")
    place, right, left = neighbours(n)
    greet(n_tp, right, left)
    rows = gu_ref.shape[0] // n
    half = rows // 2
    tokens = mix_ref.shape[0] // n_tp
    sets = ((gu_ref, gu_slots, gu_out), (dn_ref, dn_slots, dn_out))

    def local(step, way):
        if way == 0:
            owner = ring_index(lax.rem(place - step - 1 + n, n), n)
        else:
            owner = ring_index(lax.rem(place + step + 1, n), n)
        return pl.ds(pl.multiple_of(owner * rows + way * half, half), half)

    def piece(step, c, way, first, landed=False):
        partial, slots, _ = sets[c]
        source = partial.at[local(0, way)] if first else slots.at[way, step if landed else step - 1]
        return pltpu.make_async_remote_copy(
            src_ref=source,
            dst_ref=slots.at[way, step],
            send_sem=send_sem.at[step, c, way],
            recv_sem=recv_sem.at[step, c, way],
            device_id=((left if way else right), me_tp),
            device_id_type=MESH,
        )

    def gain_piece(step):
        return pltpu.make_async_remote_copy(
            src_ref=gain_slots.at[ring_index(lax.rem(place - step + n, n), n)],
            dst_ref=gain_slots.at[ring_index(lax.rem(place - step + n, n), n)],
            send_sem=gain_send.at[step],
            recv_sem=gain_recv.at[step],
            device_id=(right, me_tp),
            device_id_type=MESH,
        )

    gain_slots[me_fs] = gain_ref[...]
    for c in range(2):
        for way in range(2):
            piece(0, c, way, True).start()
    tp_copies = []
    for a, (source, target) in enumerate(((dnorm_ref, dnorm_out), (mix_ref, mix_out))):
        for away in range(1, n_tp):
            peer = lax.rem(me_tp + away, n_tp)
            copy = pltpu.make_async_remote_copy(
                src_ref=source.at[pl.ds(pl.multiple_of(peer * tokens, tokens), tokens)],
                dst_ref=target.at[away - 1],
                send_sem=tp_send.at[a, away - 1],
                recv_sem=tp_recv.at[a, away - 1],
                device_id=(me_fs, peer),
                device_id_type=MESH,
            )
            copy.start()
            tp_copies.append(copy)
    gain_piece(0).start()

    def body(step, carry):
        for c in range(2):
            partial, slots, _ = sets[c]
            for way in range(2):
                piece(step - 1, c, way, False, True).wait_recv()
                slots[way, step - 1] = (
                    slots[way, step - 1].astype(jnp.float32)
                    + partial[local(step, way), :].astype(jnp.float32)
                ).astype(jnp.bfloat16)
                piece(step, c, way, False).start()
        gain_piece(step - 1).wait_recv()
        gain_piece(step).start()
        return carry

    lax.fori_loop(1, n - 1, body, 0)
    gain_piece(n - 2).wait_recv()
    total = gain_slots[0]
    for k in range(1, n):
        total = total + gain_slots[k]
    gain_tp[me_tp] = total
    last = []
    for away in range(1, n_tp):
        peer = lax.rem(me_tp + away, n_tp)
        copy = pltpu.make_async_remote_copy(
            src_ref=gain_tp.at[me_tp],
            dst_ref=gain_tp.at[me_tp],
            send_sem=last_send.at[away - 1],
            recv_sem=last_recv.at[away - 1],
            device_id=(me_fs, peer),
            device_id_type=MESH,
        )
        copy.start()
        last.append(copy)
    for c in range(2):
        partial, slots, out = sets[c]
        for way in range(2):
            piece(n - 2, c, way, False, True).wait_recv()
            out[pl.ds(way * half, half), :] = slots[way, n - 2].astype(jnp.float32) + partial[
                local(n - 1, way), :
            ].astype(jnp.float32)
            piece(0, c, way, True).wait_send()
    for copy in last:
        copy.wait()
    total = gain_tp[0]
    for k in range(1, n_tp):
        total = total + gain_tp[k]
    gain_out[...] = total

    def drain(step, carry):
        for c in range(2):
            for way in range(2):
                piece(step, c, way, False).wait_send()
        gain_piece(step).wait_send()
        return carry

    gain_piece(0).wait_send()
    lax.fori_loop(1, n - 1, drain, 0)
    for copy in tp_copies:
        copy.wait()


def reduce(n, n_tp, gu, dn, mix, dnorm, gain):
    rows = gu.shape[0] // n
    half = rows // 2
    tokens = mix.shape[0] // n_tp
    vmem = pl.BlockSpec(memory_space=pltpu.VMEM)
    hbm = pl.BlockSpec(memory_space=pl.ANY)
    f32, bf16 = jnp.float32, jnp.bfloat16
    return pl.pallas_call(
        functools.partial(reduce_kernel, n, n_tp),
        out_shape=[
            jax.ShapeDtypeStruct((rows, gu.shape[1]), f32),
            jax.ShapeDtypeStruct((rows, dn.shape[1]), f32),
            jax.ShapeDtypeStruct((n_tp - 1, tokens, mix.shape[1]), bf16),
            jax.ShapeDtypeStruct((n_tp - 1, tokens, mix.shape[1]), bf16),
            jax.ShapeDtypeStruct(gain.shape, f32),
        ],
        in_specs=[vmem, vmem, hbm, hbm, vmem],
        out_specs=[vmem, vmem, hbm, hbm, vmem],
        scratch_shapes=[
            pltpu.VMEM((2, n - 1, half, gu.shape[1]), bf16),
            pltpu.VMEM((2, n - 1, half, dn.shape[1]), bf16),
            pltpu.VMEM((n,) + gain.shape, f32),
            pltpu.VMEM((n_tp,) + gain.shape, f32),
            pltpu.SemaphoreType.DMA((n - 1, 2, 2)),
            pltpu.SemaphoreType.DMA((n - 1, 2, 2)),
            pltpu.SemaphoreType.DMA((n - 1,)),
            pltpu.SemaphoreType.DMA((n - 1,)),
            pltpu.SemaphoreType.DMA((2, n_tp - 1)),
            pltpu.SemaphoreType.DMA((2, n_tp - 1)),
            pltpu.SemaphoreType.DMA((n_tp - 1,)),
            pltpu.SemaphoreType.DMA((n_tp - 1,)),
        ],
        compiler_params=pltpu.CompilerParams(
            collective_id=1, has_side_effects=True, vmem_limit_bytes=VMEM_LIMIT
        ),
    )(gu, dn, mix, dnorm, gain)


def normalize(source, gain_f):
    values = source.astype(jnp.float32)
    scale = lax.rsqrt(jnp.mean(values * values, axis=-1, keepdims=True) + epsilon)
    return ((values * scale * gain_f).astype(jnp.bfloat16), scale, values)


def times_transposed(left, right):
    return lax.dot_general(
        left, right, (((1,), (1,)), ((), ())), preferred_element_type=jnp.float32
    )


def column_product(left, right):
    return lax.dot_general(
        left, right, (((0,), (0,)), ((), ())), preferred_element_type=jnp.float32
    )


def per_device(
    n,
    n_tp,
    late_input,
    norm_gain,
    gate_weight,
    up_weight,
    down_weight,
    early_input,
    cotangent,
    gate_sum,
    up_sum,
    down_sum,
    gain_sum,
):
    gain_f = norm_gain.astype(jnp.float32)
    width = gate_weight.shape[1]
    depth = late_input.shape[1]
    tokens = late_input.shape[0]
    normed, _, values = normalize(late_input, gain_f)
    normed_e, scale_e, values_e = normalize(early_input, gain_f)
    gu = jnp.concatenate([gate_weight, up_weight], axis=1)
    gu_all, down_all, late_all, early_all, cot_all = gather(
        n, n_tp, gu, down_weight, normed, normed_e, cotangent
    )
    both_e = jnp.dot(early_all, gu_all, preferred_element_type=jnp.float32)
    gate_e, upper_e = both_e[:, :width], both_e[:, width:]
    sigma_e = jax.nn.sigmoid(gate_e)
    hidden_e = (gate_e * sigma_e * upper_e).astype(jnp.bfloat16)
    d_hidden = 0.5 * jnp.dot(cot_all, down_all, preferred_element_type=jnp.float32)
    d_gate = (d_hidden * upper_e * sigma_e * (1.0 + gate_e * (1.0 - sigma_e))).astype(jnp.bfloat16)
    d_up = (d_hidden * gate_e * sigma_e).astype(jnp.bfloat16)
    d_both = jnp.concatenate([d_gate, d_up], axis=1)
    d_part = times_transposed(d_both, gu_all).astype(jnp.bfloat16)
    gain_part = (
        jnp.sum(d_part.astype(jnp.float32) * early_all.astype(jnp.float32), axis=0) / gain_f
    )
    gu_part = column_product(early_all, d_both).astype(jnp.bfloat16)
    down_part = (0.5 * column_product(cot_all, hidden_e)).astype(jnp.bfloat16)
    both = jnp.dot(late_all, gu_all, preferred_element_type=jnp.float32)
    hidden = (jax.nn.silu(both[:, :width]) * both[:, width:]).astype(jnp.bfloat16)
    mix_part = times_transposed(hidden, down_all).astype(jnp.bfloat16)
    gu_grad, down_grad, mix_got, d_got, gain_total = reduce(
        n, n_tp, gu_part, down_part, mix_part, d_part, gain_part.reshape(8, depth // 8)
    )
    start = lax.axis_index("tp") * tokens

    def gathered(part, got):
        total = lax.dynamic_slice_in_dim(part, start, tokens, 0).astype(jnp.float32)
        for k in range(n_tp - 1):
            total = total + got[k].astype(jnp.float32)
        return total

    late_out = (values + 0.5 * gathered(mix_part, mix_got)).astype(jnp.bfloat16)
    scaled_grad = gathered(d_part, d_got) * gain_f
    early_grad = (
        cotangent.astype(jnp.float32)
        + scale_e * scaled_grad
        - values_e * scale_e**3 * jnp.mean(values_e * scaled_grad, axis=-1, keepdims=True)
    ).astype(jnp.bfloat16)
    return (
        late_out,
        early_grad,
        gate_sum + gu_grad[:, :width],
        up_sum + gu_grad[:, width:],
        down_sum + down_grad,
        gain_sum + gain_total.reshape(depth),
    )


def solution(mesh):
    token = P(("fs", "tp"), None)
    weight = P("fs", "tp")
    return jax.shard_map(
        functools.partial(per_device, mesh.shape["fs"], mesh.shape["tp"]),
        mesh=mesh,
        in_specs=(token, P(), weight, weight, weight, token, token, weight, weight, weight, P()),
        out_specs=(token, token, weight, weight, weight, P()),
        check_vma=False,
    )
```

```python
import functools

import jax
import jax.numpy as jnp
from jax import lax
from jax.experimental import pallas as pl
from jax.experimental.pallas import tpu as pltpu
from jax.sharding import PartitionSpec as P

epsilon = 1e-05
MESH = pl.DeviceIdType.MESH
VMEM_LIMIT = 60 * 1024 * 1024


def ring_place(index, n):
    odd = lax.rem(index, 2)
    half = index // 2
    return (1 - odd) * half + odd * (n - 1 - half)


def ring_index(place, n):
    back = place // (n // 2)
    return (1 - back) * (2 * place) + back * (2 * (n - 1 - place) + 1)


def neighbours(n):
    place = ring_place(lax.axis_index("fs"), n)
    right = ring_index(lax.rem(place + 1, n), n)
    left = ring_index(lax.rem(place + n - 1, n), n)
    return place, right, left


def greet(n_tp, right, left):
    me_tp = lax.axis_index("tp")
    barrier = pltpu.get_barrier_semaphore()
    for target in (right, left):
        pl.semaphore_signal(barrier, inc=1, device_id=(target, me_tp), device_id_type=MESH)
    for away in range(1, n_tp):
        peer = lax.rem(me_tp + away, n_tp)
        pl.semaphore_signal(
            barrier, inc=1, device_id=(lax.axis_index("fs"), peer), device_id_type=MESH
        )
    pl.semaphore_wait(barrier, 2 + n_tp - 1)


def gather_kernel(n, n_tp, *refs):
    gate_in, up_in, dn_ref, late_in, early_in, cot_ref, gain_ref = refs[:7]
    gu_all, dn_all, late_all, early_all, cot_all = refs[7:12]
    gate_buf, up_buf, gu_ref, dn_buf, late_buf, early_buf, cot_buf, late_ref, early_ref = refs[12:21]
    send_sem, recv_sem, tp_send, tp_recv, own_sem, in_sem = refs[21:]
    width = gate_in.shape[1]
    loads = [
        pltpu.make_async_copy(source, target, in_sem.at[k])
        for k, (source, target) in enumerate(
            (
                (gate_in, gate_buf),
                (up_in, up_buf),
                (early_in, early_buf),
                (late_in, late_buf),
                (dn_ref, dn_buf),
                (cot_ref, cot_buf),
            )
        )
    ]
    for copy in loads:
        copy.start()
    me_fs, me_tp = lax.axis_index("fs"), lax.axis_index("tp")
    place, right, left = neighbours(n)
    greet(n_tp, right, left)
    rows = gate_in.shape[0]
    half = rows // 2
    tokens = late_in.shape[0]
    pairs = ((gu_ref, gu_all), (dn_ref, dn_all))

    def window(owner, way):
        return pl.ds(pl.multiple_of(owner * rows + way * half, half), half)

    def piece(step, c, way, first):
        block, whole = pairs[c]
        if way == 0:
            owner = ring_index(lax.rem(place - step + n, n), n)
            target = right
        else:
            owner = ring_index(lax.rem(place + step, n), n)
            target = left
        spot = whole.at[window(owner, way)]
        source = block.at[pl.ds(way * half, half)] if first else spot
        return pltpu.make_async_remote_copy(
            src_ref=source,
            dst_ref=spot,
            send_sem=send_sem.at[step, c, way],
            recv_sem=recv_sem.at[step, c, way],
            device_id=(target, me_tp),
            device_id_type=MESH,
        )

    mine = pl.ds(pl.multiple_of(me_tp * tokens, tokens), tokens)
    token_pairs = ((early_ref, early_all), (cot_ref, cot_all), (late_ref, late_all))

    def spread(a):
        block, whole = token_pairs[a]
        copies = []
        for away in range(1, n_tp):
            peer = lax.rem(me_tp + away, n_tp)
            copy = pltpu.make_async_remote_copy(
                src_ref=block,
                dst_ref=whole.at[mine],
                send_sem=tp_send.at[a, away - 1],
                recv_sem=tp_recv.at[a, away - 1],
                device_id=(me_fs, peer),
                device_id_type=MESH,
            )
            copy.start()
            copies.append(copy)
        return copies

    def norm(source, target):
        def part(k, carry):
            some = pl.ds(pl.multiple_of(k * 16, 16), 16)
            values = source[some, :].astype(jnp.float32)
            scale = lax.rsqrt(jnp.mean(values * values, axis=-1, keepdims=True) + epsilon)
            target[some, :] = (values * scale * gain_ref[...]).astype(jnp.bfloat16)
            return carry

        lax.fori_loop(0, tokens // 16, part, 0)

    for way in range(2):
        piece(0, 1, way, True).start()
    token_copies = spread(1)
    loads[0].wait()
    loads[1].wait()
    gu_ref[:, :width] = gate_buf[...]
    gu_ref[:, width:] = up_buf[...]
    for way in range(2):
        piece(0, 0, way, True).start()
    loads[2].wait()
    norm(early_buf, early_ref)
    token_copies += spread(0)
    loads[3].wait()
    norm(late_buf, late_ref)
    token_copies += spread(2)
    loads[4].wait()
    loads[5].wait()
    own = []
    sources = (early_ref, cot_buf, late_ref)
    for a in range(3):
        own.append(
            pltpu.make_async_copy(sources[a], token_pairs[a][1].at[mine], own_sem.at[a])
        )
    for c, (block, whole) in enumerate(((gu_ref, gu_all), (dn_buf, dn_all))):
        own.append(
            pltpu.make_async_copy(
                block,
                whole.at[pl.ds(pl.multiple_of(me_fs * rows, rows), rows)],
                own_sem.at[3 + c],
            )
        )
    for copy in own:
        copy.start()

    def body(step, carry):
        for c in (1, 0):
            for way in range(2):
                piece(step - 1, c, way, False).wait_recv()
                piece(step, c, way, False).start()
        return carry

    lax.fori_loop(1, n - 1, body, 0)
    for c in (1, 0):
        for way in range(2):
            piece(n - 2, c, way, False).wait_recv()
            piece(0, c, way, True).wait_send()

    def drain(step, carry):
        for c in (1, 0):
            for way in range(2):
                piece(step, c, way, False).wait_send()
        return carry

    lax.fori_loop(1, n - 1, drain, 0)
    for copy in own:
        copy.wait()
    for copy in token_copies:
        copy.wait()


def gather(n, n_tp, gate, up, dn, late, early, cot, gain):
    rows, width = gate.shape
    tokens, depth = late.shape
    vmem = pl.BlockSpec(memory_space=pltpu.VMEM)
    hbm = pl.BlockSpec(memory_space=pl.ANY)
    bf16 = jnp.bfloat16
    return pl.pallas_call(
        functools.partial(gather_kernel, n, n_tp),
        out_shape=[
            jax.ShapeDtypeStruct((n * rows, 2 * width), bf16),
            jax.ShapeDtypeStruct((n * rows, width), bf16),
        ]
        + [jax.ShapeDtypeStruct((n_tp * tokens, depth), bf16)] * 3,
        in_specs=[hbm] * 6 + [vmem],
        out_specs=[hbm] * 5,
        scratch_shapes=[
            pltpu.VMEM((rows, width), bf16),
            pltpu.VMEM((rows, width), bf16),
            pltpu.VMEM((rows, 2 * width), bf16),
            pltpu.VMEM((rows, width), bf16),
        ]
        + [pltpu.VMEM((tokens, depth), bf16)] * 5
        + [
            pltpu.SemaphoreType.DMA((n - 1, 2, 2)),
            pltpu.SemaphoreType.DMA((n - 1, 2, 2)),
            pltpu.SemaphoreType.DMA((3, n_tp - 1)),
            pltpu.SemaphoreType.DMA((3, n_tp - 1)),
            pltpu.SemaphoreType.DMA((5,)),
            pltpu.SemaphoreType.DMA((6,)),
        ],
        compiler_params=pltpu.CompilerParams(
            collective_id=0, has_side_effects=True, vmem_limit_bytes=VMEM_LIMIT
        ),
    )(gate, up, dn, late, early, cot, gain)


def reduce_kernel(n, n_tp, *refs):
    gu_ref, dn_ref, both_ref, gain_ref, gu_in, dn_in, late_in, early_in = refs[:8]
    gu_out, dn_out, mix_out, dnorm_out, gain_out = refs[8:13]
    gu_slots, dn_slots, gain_slots, gain_tp = refs[13:17]
    gu_all, dn_all, late_all, early_all, mix_ref, dnorm_ref, gain_sum = refs[17:24]
    send_sem, recv_sem, gain_send, gain_recv, tp_send, tp_recv, last_send, last_recv = refs[24:32]
    in_sem, own_sem = refs[32:]
    loads = [
        pltpu.make_async_copy(source, target, in_sem.at[k])
        for k, (source, target) in enumerate(
            ((gu_in, gu_all), (early_in, early_all), (late_in, late_all), (dn_in, dn_all))
        )
    ]
    for copy in loads:
        copy.start()
    me_fs, me_tp = lax.axis_index("fs"), lax.axis_index("tp")
    place, right, left = neighbours(n)
    barrier = pltpu.get_barrier_semaphore()

    def greet_fs(away, carry):
        target = lax.rem(me_fs + away, n)
        pl.semaphore_signal(barrier, inc=1, device_id=(target, me_tp), device_id_type=MESH)
        return carry

    lax.fori_loop(1, n, greet_fs, 0)
    for away in range(1, n_tp):
        peer = lax.rem(me_tp + away, n_tp)
        pl.semaphore_signal(barrier, inc=1, device_id=(me_fs, peer), device_id_type=MESH)
    pl.semaphore_wait(barrier, n - 1 + n_tp - 1)
    width = dn_all.shape[1]
    rows = gu_ref.shape[0] // n
    half = rows // 2
    tokens = late_all.shape[0] // n_tp
    sets = ((gu_ref, gu_slots, gu_out), (dn_ref, dn_slots, dn_out))

    def local(step, way):
        if way == 0:
            owner = ring_index(lax.rem(place - step - 1 + n, n), n)
        else:
            owner = ring_index(lax.rem(place + step + 1, n), n)
        return pl.ds(pl.multiple_of(owner * rows + way * half, half), half)

    def piece(step, c, way, first, landed=False):
        partial, slots, _ = sets[c]
        source = partial.at[local(0, way)] if first else slots.at[way, step if landed else step - 1]
        return pltpu.make_async_remote_copy(
            src_ref=source,
            dst_ref=slots.at[way, step],
            send_sem=send_sem.at[step, c, way],
            recv_sem=recv_sem.at[step, c, way],
            device_id=((left if way else right), me_tp),
            device_id_type=MESH,
        )

    def gain_piece(away):
        return pltpu.make_async_remote_copy(
            src_ref=gain_slots.at[me_fs],
            dst_ref=gain_slots.at[me_fs],
            send_sem=gain_send.at[away - 1],
            recv_sem=gain_recv.at[away - 1],
            device_id=(lax.rem(me_fs + away, n), me_tp),
            device_id_type=MESH,
        )

    results = ((dnorm_ref, dnorm_out), (mix_ref, mix_out))

    def share(a, away):
        source, target = results[a]
        return pltpu.make_async_remote_copy(
            src_ref=source.at[away - 1],
            dst_ref=target.at[away - 1],
            send_sem=tp_send.at[a, away - 1],
            recv_sem=tp_recv.at[a, away - 1],
            device_id=(me_fs, lax.rem(me_tp + away, n_tp)),
            device_id_type=MESH,
        )

    def keep(a):
        source, target = results[a]
        return pltpu.make_async_copy(source.at[n_tp - 1], target.at[n_tp - 1], own_sem.at[a])

    def block_of(away):
        return pl.ds(pl.multiple_of(lax.rem(me_tp + away, n_tp) * tokens, tokens), tokens)

    def grad_block(away):
        some = block_of(away)
        part = lax.dot_general(
            both_ref[some, :],
            gu_all[...],
            (((1,), (1,)), ((), ())),
            preferred_element_type=jnp.float32,
        ).astype(jnp.bfloat16)
        dnorm_ref[away - 1] = part
        gain_sum[...] += jnp.sum(
            part.astype(jnp.float32) * early_all[some, :].astype(jnp.float32),
            axis=0,
            keepdims=True,
        )

    def late_block(away):
        both = jnp.dot(
            late_all[block_of(away), :], gu_all[...], preferred_element_type=jnp.float32
        )
        gate = both[:, :width]
        hidden = (gate / (1.0 + jnp.exp(-gate)) * both[:, width:]).astype(jnp.bfloat16)
        mix_ref[away - 1] = lax.dot_general(
            hidden, dn_all[...], (((1,), (1,)), ((), ())), preferred_element_type=jnp.float32
        ).astype(jnp.bfloat16)

    for c in range(2):
        for way in range(2):
            piece(0, c, way, True).start()
    gain_sum[...] = jnp.zeros_like(gain_sum)
    for copy in loads:
        copy.wait()

    def body(step, carry):
        for c in range(2):
            partial, slots, _ = sets[c]
            for way in range(2):
                piece(step - 1, c, way, False, True).wait_recv()
                slots[way, step - 1] = (
                    slots[way, step - 1].astype(jnp.float32)
                    + partial[local(step, way), :].astype(jnp.float32)
                ).astype(jnp.bfloat16)
                piece(step, c, way, False).start()

            @pl.when(step <= n_tp)
            def _():
                (grad_block, late_block)[c](step)

            @pl.when(step < n_tp)
            def _():
                share(c, step).start()

            @pl.when(step == n_tp)
            def _():
                keep(c).start()

        @pl.when(step == n_tp)
        def _():
            gain_slots[me_fs] = gain_sum[...] / gain_ref[...]

            def send(away, inner):
                gain_piece(away).start()
                return inner

            lax.fori_loop(1, n, send, 0)

        return carry

    lax.fori_loop(1, n - 1, body, 0)

    def settle(away, inner):
        gain_piece(away).wait()
        return inner

    lax.fori_loop(1, n, settle, 0)
    gain_tp[me_tp] = lax.fori_loop(
        1, n, lambda k, total: total + gain_slots[k], gain_slots[0]
    )
    last = []
    for away in range(1, n_tp):
        peer = lax.rem(me_tp + away, n_tp)
        copy = pltpu.make_async_remote_copy(
            src_ref=gain_tp.at[me_tp],
            dst_ref=gain_tp.at[me_tp],
            send_sem=last_send.at[away - 1],
            recv_sem=last_recv.at[away - 1],
            device_id=(me_fs, peer),
            device_id_type=MESH,
        )
        copy.start()
        last.append(copy)
    for c in range(2):
        partial, slots, out = sets[c]
        for way in range(2):
            piece(n - 2, c, way, False, True).wait_recv()
            out[pl.ds(way * half, half), :] = slots[way, n - 2].astype(jnp.float32) + partial[
                local(n - 1, way), :
            ].astype(jnp.float32)
            piece(0, c, way, True).wait_send()
    for copy in last:
        copy.wait()
    total = gain_tp[0]
    for k in range(1, n_tp):
        total = total + gain_tp[k]
    gain_out[...] = total

    def drain(step, carry):
        for c in range(2):
            for way in range(2):
                piece(step, c, way, False).wait_send()
        return carry

    lax.fori_loop(1, n - 1, drain, 0)
    for a in range(2):
        keep(a).wait()
        for away in range(1, n_tp):
            share(a, away).wait()


def reduce(n, n_tp, gu, dn, both, gain, gu_all, dn_all, late_all, early_all):
    rows = gu.shape[0] // n
    half = rows // 2
    depth = late_all.shape[1]
    tokens = late_all.shape[0] // n_tp
    vmem = pl.BlockSpec(memory_space=pltpu.VMEM)
    hbm = pl.BlockSpec(memory_space=pl.ANY)
    f32, bf16 = jnp.float32, jnp.bfloat16
    return pl.pallas_call(
        functools.partial(reduce_kernel, n, n_tp),
        out_shape=[
            jax.ShapeDtypeStruct((rows, gu.shape[1]), f32),
            jax.ShapeDtypeStruct((rows, dn.shape[1]), f32),
            jax.ShapeDtypeStruct((n_tp, tokens, depth), bf16),
            jax.ShapeDtypeStruct((n_tp, tokens, depth), bf16),
            jax.ShapeDtypeStruct(gain.shape, f32),
        ],
        in_specs=[vmem] * 4 + [hbm] * 4,
        out_specs=[vmem, vmem, hbm, hbm, vmem],
        scratch_shapes=[
            pltpu.VMEM((2, n - 1, half, gu.shape[1]), bf16),
            pltpu.VMEM((2, n - 1, half, dn.shape[1]), bf16),
            pltpu.VMEM((n,) + gain.shape, f32),
            pltpu.VMEM((n_tp,) + gain.shape, f32),
            pltpu.VMEM(gu_all.shape, bf16),
            pltpu.VMEM(dn_all.shape, bf16),
            pltpu.VMEM(late_all.shape, bf16),
            pltpu.VMEM(early_all.shape, bf16),
            pltpu.VMEM((n_tp, tokens, depth), bf16),
            pltpu.VMEM((n_tp, tokens, depth), bf16),
            pltpu.VMEM(gain.shape, f32),
            pltpu.SemaphoreType.DMA((n - 1, 2, 2)),
            pltpu.SemaphoreType.DMA((n - 1, 2, 2)),
            pltpu.SemaphoreType.DMA((n - 1,)),
            pltpu.SemaphoreType.DMA((n - 1,)),
            pltpu.SemaphoreType.DMA((2, n_tp - 1)),
            pltpu.SemaphoreType.DMA((2, n_tp - 1)),
            pltpu.SemaphoreType.DMA((n_tp - 1,)),
            pltpu.SemaphoreType.DMA((n_tp - 1,)),
            pltpu.SemaphoreType.DMA((4,)),
            pltpu.SemaphoreType.DMA((2,)),
        ],
        compiler_params=pltpu.CompilerParams(
            collective_id=1, has_side_effects=True, vmem_limit_bytes=VMEM_LIMIT
        ),
    )(gu, dn, both, gain, gu_all, dn_all, late_all, early_all)


def column_product(left, right):
    return lax.dot_general(
        left, right, (((0,), (0,)), ((), ())), preferred_element_type=jnp.float32
    )


def per_device(
    n,
    n_tp,
    late_input,
    norm_gain,
    gate_weight,
    up_weight,
    down_weight,
    early_input,
    cotangent,
    gate_sum,
    up_sum,
    down_sum,
    gain_sum,
):
    gain_f = norm_gain.astype(jnp.float32)
    width = gate_weight.shape[1]
    depth = late_input.shape[1]
    gain_row = gain_f.reshape(1, depth)
    gu_all, down_all, late_all, early_all, cot_all = gather(
        n, n_tp, gate_weight, up_weight, down_weight, late_input, early_input, cotangent, gain_row
    )
    both_e = jnp.dot(early_all, gu_all, preferred_element_type=jnp.float32)
    gate_e, upper_e = both_e[:, :width], both_e[:, width:]
    sigma_e = jax.nn.sigmoid(gate_e)
    hidden_e = (gate_e * sigma_e * upper_e).astype(jnp.bfloat16)
    d_hidden = 0.5 * jnp.dot(cot_all, down_all, preferred_element_type=jnp.float32)
    d_gate = (d_hidden * upper_e * sigma_e * (1.0 + gate_e * (1.0 - sigma_e))).astype(jnp.bfloat16)
    d_up = (d_hidden * gate_e * sigma_e).astype(jnp.bfloat16)
    d_both = jnp.concatenate([d_gate, d_up], axis=1)
    gu_part = column_product(early_all, d_both).astype(jnp.bfloat16)
    down_part = (0.5 * column_product(cot_all, hidden_e)).astype(jnp.bfloat16)
    gu_grad, down_grad, mix_got, d_got, gain_total = reduce(
        n, n_tp, gu_part, down_part, d_both, gain_row, gu_all, down_all, late_all, early_all
    )

    def gathered(got):
        total = got[0].astype(jnp.float32)
        for k in range(1, n_tp):
            total = total + got[k].astype(jnp.float32)
        return total

    values = late_input.astype(jnp.float32)
    values_e = early_input.astype(jnp.float32)
    scale_e = lax.rsqrt(jnp.mean(values_e * values_e, axis=-1, keepdims=True) + epsilon)
    late_out = (values + 0.5 * gathered(mix_got)).astype(jnp.bfloat16)
    scaled_grad = gathered(d_got) * gain_f
    early_grad = (
        cotangent.astype(jnp.float32)
        + scale_e * scaled_grad
        - values_e * scale_e**3 * jnp.mean(values_e * scaled_grad, axis=-1, keepdims=True)
    ).astype(jnp.bfloat16)
    return (
        late_out,
        early_grad,
        gate_sum + gu_grad[:, :width],
        up_sum + gu_grad[:, width:],
        down_sum + down_grad,
        gain_sum + gain_total.reshape(depth),
    )


def solution(mesh):
    token = P(("fs", "tp"), None)
    weight = P("fs", "tp")
    return jax.shard_map(
        functools.partial(per_device, mesh.shape["fs"], mesh.shape["tp"]),
        mesh=mesh,
        in_specs=(token, P(), weight, weight, weight, token, token, weight, weight, weight, P()),
        out_specs=(token, token, weight, weight, weight, P()),
        check_vma=False,
    )
```

```python
import functools

import jax
import jax.numpy as jnp
from jax import lax
from jax.experimental import pallas as pl
from jax.experimental.pallas import tpu as pltpu
from jax.sharding import PartitionSpec as P

epsilon = 1e-05
MESH = pl.DeviceIdType.MESH
VMEM_LIMIT = 60 * 1024 * 1024


def ring_place(index, n):
    odd = lax.rem(index, 2)
    half = index // 2
    return (1 - odd) * half + odd * (n - 1 - half)


def ring_index(place, n):
    back = place // (n // 2)
    return (1 - back) * (2 * place) + back * (2 * (n - 1 - place) + 1)


def neighbours(n):
    place = ring_place(lax.axis_index("fs"), n)
    right = ring_index(lax.rem(place + 1, n), n)
    left = ring_index(lax.rem(place + n - 1, n), n)
    return place, right, left


def greet(n_tp, right, left):
    me_tp = lax.axis_index("tp")
    barrier = pltpu.get_barrier_semaphore()
    for target in (right, left):
        pl.semaphore_signal(barrier, inc=1, device_id=(target, me_tp), device_id_type=MESH)
    for away in range(1, n_tp):
        peer = lax.rem(me_tp + away, n_tp)
        pl.semaphore_signal(
            barrier, inc=1, device_id=(lax.axis_index("fs"), peer), device_id_type=MESH
        )
    pl.semaphore_wait(barrier, 2 + n_tp - 1)


def gather_kernel(n, n_tp, turned, *refs):
    gate_in, up_in, dn_in, late_in, early_in, cot_ref, gain_ref = refs[:7]
    gu_all, dn_all, late_all, early_all, cot_all = refs[7:12]
    gate_buf, up_buf, gu_ref, dn_buf, dn_ref = refs[12:17]
    late_buf, early_buf, cot_buf, late_ref, early_ref = refs[17:22]
    send_sem, recv_sem, tp_send, tp_recv, own_sem, in_sem = refs[22:]
    rows, width = dn_ref.shape
    loads = [
        pltpu.make_async_copy(source, target, in_sem.at[k])
        for k, (source, target) in enumerate(
            (
                (gate_in, gate_buf),
                (up_in, up_buf),
                (early_in, early_buf),
                (late_in, late_buf),
                (dn_in, dn_buf),
                (cot_ref, cot_buf),
            )
        )
    ]
    for copy in loads:
        copy.start()
    me_fs, me_tp = lax.axis_index("fs"), lax.axis_index("tp")
    place, right, left = neighbours(n)
    greet(n_tp, right, left)
    half = rows // 2
    tokens = late_in.shape[0]
    pairs = ((gu_ref, gu_all), (dn_ref, dn_all))

    def window(owner, way):
        return pl.ds(pl.multiple_of(owner * rows + way * half, half), half)

    def piece(step, c, way, first):
        block, whole = pairs[c]
        if way == 0:
            owner = ring_index(lax.rem(place - step + n, n), n)
            target = right
        else:
            owner = ring_index(lax.rem(place + step, n), n)
            target = left
        spot = whole.at[window(owner, way)]
        source = block.at[pl.ds(way * half, half)] if first else spot
        return pltpu.make_async_remote_copy(
            src_ref=source,
            dst_ref=spot,
            send_sem=send_sem.at[step, c, way],
            recv_sem=recv_sem.at[step, c, way],
            device_id=(target, me_tp),
            device_id_type=MESH,
        )

    mine = pl.ds(pl.multiple_of(me_tp * tokens, tokens), tokens)
    token_pairs = ((early_ref, early_all), (cot_ref, cot_all), (late_ref, late_all))

    def spread(a):
        block, whole = token_pairs[a]
        copies = []
        for away in range(1, n_tp):
            peer = lax.rem(me_tp + away, n_tp)
            copy = pltpu.make_async_remote_copy(
                src_ref=block,
                dst_ref=whole.at[mine],
                send_sem=tp_send.at[a, away - 1],
                recv_sem=tp_recv.at[a, away - 1],
                device_id=(me_fs, peer),
                device_id_type=MESH,
            )
            copy.start()
            copies.append(copy)
        return copies

    def norm(source, target):
        def part(k, carry):
            some = pl.ds(pl.multiple_of(k * 16, 16), 16)
            values = source[some, :].astype(jnp.float32)
            scale = lax.rsqrt(jnp.mean(values * values, axis=-1, keepdims=True) + epsilon)
            target[some, :] = (values * scale * gain_ref[...]).astype(jnp.bfloat16)
            return carry

        lax.fori_loop(0, tokens // 16, part, 0)

    def plain(buffer):
        return buffer[...].T if turned else buffer[...]

    loads[4].wait()
    dn_ref[...] = plain(dn_buf)
    for way in range(2):
        piece(0, 1, way, True).start()
    token_copies = spread(1)
    loads[0].wait()
    loads[1].wait()
    gu_ref[:, :width] = plain(gate_buf)
    gu_ref[:, width:] = plain(up_buf)
    for way in range(2):
        piece(0, 0, way, True).start()
    loads[2].wait()
    norm(early_buf, early_ref)
    token_copies += spread(0)
    loads[3].wait()
    norm(late_buf, late_ref)
    token_copies += spread(2)
    loads[5].wait()
    own = []
    sources = (early_ref, cot_buf, late_ref)
    for a in range(3):
        own.append(
            pltpu.make_async_copy(sources[a], token_pairs[a][1].at[mine], own_sem.at[a])
        )
    for c, (block, whole) in enumerate(((gu_ref, gu_all), (dn_ref, dn_all))):
        own.append(
            pltpu.make_async_copy(
                block,
                whole.at[pl.ds(pl.multiple_of(me_fs * rows, rows), rows)],
                own_sem.at[3 + c],
            )
        )
    for copy in own:
        copy.start()

    def body(step, carry):
        for c in (1, 0):
            for way in range(2):
                piece(step - 1, c, way, False).wait_recv()
                piece(step, c, way, False).start()
        return carry

    lax.fori_loop(1, n - 1, body, 0)
    for c in (1, 0):
        for way in range(2):
            piece(n - 2, c, way, False).wait_recv()
            piece(0, c, way, True).wait_send()

    def drain(step, carry):
        for c in (1, 0):
            for way in range(2):
                piece(step, c, way, False).wait_send()
        return carry

    lax.fori_loop(1, n - 1, drain, 0)
    for copy in own:
        copy.wait()
    for copy in token_copies:
        copy.wait()


def gather(n, n_tp, turned, gate, up, dn, late, early, cot, gain):
    rows, width = gate.shape[::-1] if turned else gate.shape
    tokens, depth = late.shape
    vmem = pl.BlockSpec(memory_space=pltpu.VMEM)
    hbm = pl.BlockSpec(memory_space=pl.ANY)
    bf16 = jnp.bfloat16
    return pl.pallas_call(
        functools.partial(gather_kernel, n, n_tp, turned),
        out_shape=[
            jax.ShapeDtypeStruct((n * rows, 2 * width), bf16),
            jax.ShapeDtypeStruct((n * rows, width), bf16),
        ]
        + [jax.ShapeDtypeStruct((n_tp * tokens, depth), bf16)] * 3,
        in_specs=[hbm] * 6 + [vmem],
        out_specs=[hbm] * 5,
        scratch_shapes=[
            pltpu.VMEM(gate.shape, bf16),
            pltpu.VMEM(gate.shape, bf16),
            pltpu.VMEM((rows, 2 * width), bf16),
            pltpu.VMEM(gate.shape, bf16),
            pltpu.VMEM((rows, width), bf16),
        ]
        + [pltpu.VMEM((tokens, depth), bf16)] * 5
        + [
            pltpu.SemaphoreType.DMA((n - 1, 2, 2)),
            pltpu.SemaphoreType.DMA((n - 1, 2, 2)),
            pltpu.SemaphoreType.DMA((3, n_tp - 1)),
            pltpu.SemaphoreType.DMA((3, n_tp - 1)),
            pltpu.SemaphoreType.DMA((5,)),
            pltpu.SemaphoreType.DMA((6,)),
        ],
        compiler_params=pltpu.CompilerParams(
            collective_id=0, has_side_effects=True, vmem_limit_bytes=VMEM_LIMIT
        ),
    )(gate, up, dn, late, early, cot, gain)


def reduce_kernel(n, n_tp, turned, *refs):
    early_side, cot_side, both_ref, hid_ref, gain_ref, early_all, gu_in, dn_in, late_in = refs[:9]
    gu_out, dn_out, mix_out, dnorm_out, gain_out = refs[9:14]
    gu_slots, dn_slots, gain_slots, gain_tp, gu_first, dn_first = refs[14:20]
    gu_all, dn_all, late_all, mix_ref, dnorm_ref, gain_sum = refs[20:26]
    send_sem, recv_sem, gain_send, gain_recv, tp_send, tp_recv, last_send, last_recv = refs[26:34]
    in_sem, own_sem = refs[34:]
    loads = [
        pltpu.make_async_copy(source, target, in_sem.at[k])
        for k, (source, target) in enumerate(
            ((gu_in, gu_all), (late_in, late_all), (dn_in, dn_all))
        )
    ]
    for copy in loads:
        copy.start()
    me_fs, me_tp = lax.axis_index("fs"), lax.axis_index("tp")
    place, right, left = neighbours(n)
    barrier = pltpu.get_barrier_semaphore()

    def greet_fs(away, carry):
        target = lax.rem(me_fs + away, n)
        pl.semaphore_signal(barrier, inc=1, device_id=(target, me_tp), device_id_type=MESH)
        return carry

    lax.fori_loop(1, n, greet_fs, 0)
    for away in range(1, n_tp):
        peer = lax.rem(me_tp + away, n_tp)
        pl.semaphore_signal(barrier, inc=1, device_id=(me_fs, peer), device_id_type=MESH)
    pl.semaphore_wait(barrier, n - 1 + n_tp - 1)
    width = dn_all.shape[1]
    half = gu_first.shape[1]
    rows = 2 * half
    tokens = late_all.shape[0] // n_tp
    sets = ((gu_first, gu_slots), (dn_first, dn_slots))
    factors = ((early_side, both_ref, 1.0), (cot_side, hid_ref, 0.5))

    def local(step, way):
        if way == 0:
            owner = ring_index(lax.rem(place - step - 1 + n, n), n)
        else:
            owner = ring_index(lax.rem(place + step + 1, n), n)
        return pl.ds(pl.multiple_of(owner * rows + way * half, half), half)

    def product(step, c, way):
        side, other, factor = factors[c]
        if turned:
            left, contract = side[:, local(step, way)], 0
        else:
            left, contract = side[local(step, way), :], 1
        return factor * lax.dot_general(
            left,
            other[...],
            (((contract,), (0,)), ((), ())),
            preferred_element_type=jnp.float32,
        )

    def piece(step, c, way, first, landed=False):
        start, slots = sets[c]
        source = start.at[way] if first else slots.at[way, step if landed else step - 1]
        return pltpu.make_async_remote_copy(
            src_ref=source,
            dst_ref=slots.at[way, step],
            send_sem=send_sem.at[step, c, way],
            recv_sem=recv_sem.at[step, c, way],
            device_id=((left if way else right), me_tp),
            device_id_type=MESH,
        )

    def gain_piece(away):
        return pltpu.make_async_remote_copy(
            src_ref=gain_slots.at[me_fs],
            dst_ref=gain_slots.at[me_fs],
            send_sem=gain_send.at[away - 1],
            recv_sem=gain_recv.at[away - 1],
            device_id=(lax.rem(me_fs + away, n), me_tp),
            device_id_type=MESH,
        )

    results = ((dnorm_ref, dnorm_out), (mix_ref, mix_out))

    def share(a, away):
        source, target = results[a]
        return pltpu.make_async_remote_copy(
            src_ref=source.at[away - 1],
            dst_ref=target.at[away - 1],
            send_sem=tp_send.at[a, away - 1],
            recv_sem=tp_recv.at[a, away - 1],
            device_id=(me_fs, lax.rem(me_tp + away, n_tp)),
            device_id_type=MESH,
        )

    def keep(a):
        source, target = results[a]
        return pltpu.make_async_copy(source.at[n_tp - 1], target.at[n_tp - 1], own_sem.at[a])

    def block_of(away):
        return pl.ds(pl.multiple_of(lax.rem(me_tp + away, n_tp) * tokens, tokens), tokens)

    def grad_block(away):
        some = block_of(away)
        part = lax.dot_general(
            both_ref[some, :],
            gu_all[...],
            (((1,), (1,)), ((), ())),
            preferred_element_type=jnp.float32,
        ).astype(jnp.bfloat16)
        dnorm_ref[away - 1] = part
        gain_sum[...] += jnp.sum(
            part.astype(jnp.float32) * early_all[some, :].astype(jnp.float32),
            axis=0,
            keepdims=True,
        )

    def late_block(away):
        both = jnp.dot(
            late_all[block_of(away), :], gu_all[...], preferred_element_type=jnp.float32
        )
        gate = both[:, :width]
        hidden = (gate / (1.0 + jnp.exp(-gate)) * both[:, width:]).astype(jnp.bfloat16)
        mix_ref[away - 1] = lax.dot_general(
            hidden, dn_all[...], (((1,), (1,)), ((), ())), preferred_element_type=jnp.float32
        ).astype(jnp.bfloat16)

    for c in range(2):
        for way in range(2):
            sets[c][0][way] = product(0, c, way).astype(jnp.bfloat16)
            piece(0, c, way, True).start()
    gain_sum[...] = jnp.zeros_like(gain_sum)
    for copy in loads:
        copy.wait()

    def body(step, carry):
        for c in range(2):
            slots = sets[c][1]
            for way in range(2):
                term = product(step, c, way)
                piece(step - 1, c, way, False, True).wait_recv()
                slots[way, step - 1] = (
                    slots[way, step - 1].astype(jnp.float32) + term
                ).astype(jnp.bfloat16)
                piece(step, c, way, False).start()

            @pl.when(step <= n_tp)
            def _():
                (grad_block, late_block)[c](step)

            @pl.when(step < n_tp)
            def _():
                share(c, step).start()

            @pl.when(step == n_tp)
            def _():
                keep(c).start()

        @pl.when(step == n_tp)
        def _():
            gain_slots[me_fs] = gain_sum[...] / gain_ref[...]

            def send(away, inner):
                gain_piece(away).start()
                return inner

            lax.fori_loop(1, n, send, 0)

        return carry

    lax.fori_loop(1, n - 1, body, 0)

    def settle(away, inner):
        gain_piece(away).wait()
        return inner

    lax.fori_loop(1, n, settle, 0)
    gain_tp[me_tp] = lax.fori_loop(
        1, n, lambda k, total: total + gain_slots[k], gain_slots[0]
    )
    last = []
    for away in range(1, n_tp):
        peer = lax.rem(me_tp + away, n_tp)
        copy = pltpu.make_async_remote_copy(
            src_ref=gain_tp.at[me_tp],
            dst_ref=gain_tp.at[me_tp],
            send_sem=last_send.at[away - 1],
            recv_sem=last_recv.at[away - 1],
            device_id=(me_fs, peer),
            device_id_type=MESH,
        )
        copy.start()
        last.append(copy)
    for c in range(2):
        slots = sets[c][1]
        for way in range(2):
            term = product(n - 1, c, way)
            piece(n - 2, c, way, False, True).wait_recv()
            total = slots[way, n - 2].astype(jnp.float32) + term
            out = (gu_out, dn_out)[c]
            if turned:
                out[:, pl.ds(way * half, half)] = total.T
            else:
                out[pl.ds(way * half, half), :] = total
            piece(0, c, way, True).wait_send()
    for copy in last:
        copy.wait()
    total = gain_tp[0]
    for k in range(1, n_tp):
        total = total + gain_tp[k]
    gain_out[...] = total

    def drain(step, carry):
        for c in range(2):
            for way in range(2):
                piece(step, c, way, False).wait_send()
        return carry

    lax.fori_loop(1, n - 1, drain, 0)
    for a in range(2):
        keep(a).wait()
        for away in range(1, n_tp):
            share(a, away).wait()


def reduce(n, n_tp, turned, early_side, cot_side, both, hid, gain, early_all, gu_all, dn_all, late_all):
    rows = gu_all.shape[0] // n
    half = rows // 2
    width = dn_all.shape[1]
    shapes = [(rows, 2 * width), (rows, width)]
    if turned:
        shapes = [shape[::-1] for shape in shapes]
    depth = late_all.shape[1]
    tokens = late_all.shape[0] // n_tp
    vmem = pl.BlockSpec(memory_space=pltpu.VMEM)
    hbm = pl.BlockSpec(memory_space=pl.ANY)
    f32, bf16 = jnp.float32, jnp.bfloat16
    return pl.pallas_call(
        functools.partial(reduce_kernel, n, n_tp, turned),
        out_shape=[
            jax.ShapeDtypeStruct(shapes[0], f32),
            jax.ShapeDtypeStruct(shapes[1], f32),
            jax.ShapeDtypeStruct((n_tp, tokens, depth), bf16),
            jax.ShapeDtypeStruct((n_tp, tokens, depth), bf16),
            jax.ShapeDtypeStruct(gain.shape, f32),
        ],
        in_specs=[vmem] * 6 + [hbm] * 3,
        out_specs=[vmem, vmem, hbm, hbm, vmem],
        scratch_shapes=[
            pltpu.VMEM((2, n - 1, half, 2 * width), bf16),
            pltpu.VMEM((2, n - 1, half, width), bf16),
            pltpu.VMEM((n,) + gain.shape, f32),
            pltpu.VMEM((n_tp,) + gain.shape, f32),
            pltpu.VMEM((2, half, 2 * width), bf16),
            pltpu.VMEM((2, half, width), bf16),
            pltpu.VMEM(gu_all.shape, bf16),
            pltpu.VMEM(dn_all.shape, bf16),
            pltpu.VMEM(late_all.shape, bf16),
            pltpu.VMEM((n_tp, tokens, depth), bf16),
            pltpu.VMEM((n_tp, tokens, depth), bf16),
            pltpu.VMEM(gain.shape, f32),
            pltpu.SemaphoreType.DMA((n - 1, 2, 2)),
            pltpu.SemaphoreType.DMA((n - 1, 2, 2)),
            pltpu.SemaphoreType.DMA((n - 1,)),
            pltpu.SemaphoreType.DMA((n - 1,)),
            pltpu.SemaphoreType.DMA((2, n_tp - 1)),
            pltpu.SemaphoreType.DMA((2, n_tp - 1)),
            pltpu.SemaphoreType.DMA((n_tp - 1,)),
            pltpu.SemaphoreType.DMA((n_tp - 1,)),
            pltpu.SemaphoreType.DMA((3,)),
            pltpu.SemaphoreType.DMA((2,)),
        ],
        compiler_params=pltpu.CompilerParams(
            collective_id=1, has_side_effects=True, vmem_limit_bytes=VMEM_LIMIT
        ),
    )(early_side, cot_side, both, hid, gain, early_all, gu_all, dn_all, late_all)


def per_device(
    n,
    n_tp,
    late_input,
    norm_gain,
    gate_weight,
    up_weight,
    down_weight,
    early_input,
    cotangent,
    gate_sum,
    up_sum,
    down_sum,
    gain_sum,
):
    gain_f = norm_gain.astype(jnp.float32)
    width = gate_weight.shape[1]
    depth = late_input.shape[1]
    turned = gate_weight.shape[0] % 256 == 0
    weights = [gate_weight, up_weight, down_weight]
    if turned:
        weights = [weight.T for weight in weights]
    gain_row = gain_f.reshape(1, depth)
    gu_all, down_all, late_all, early_all, cot_all = gather(
        n, n_tp, turned, *weights, late_input, early_input, cotangent, gain_row
    )
    both_e = jnp.dot(early_all, gu_all, preferred_element_type=jnp.float32)
    gate_e, upper_e = both_e[:, :width], both_e[:, width:]
    sigma_e = jax.nn.sigmoid(gate_e)
    hidden_e = (gate_e * sigma_e * upper_e).astype(jnp.bfloat16)
    d_hidden = 0.5 * jnp.dot(cot_all, down_all, preferred_element_type=jnp.float32)
    d_gate = (d_hidden * upper_e * sigma_e * (1.0 + gate_e * (1.0 - sigma_e))).astype(jnp.bfloat16)
    d_up = (d_hidden * gate_e * sigma_e).astype(jnp.bfloat16)
    d_both = jnp.concatenate([d_gate, d_up], axis=1)
    sides = (early_all, cot_all) if turned else (early_all.T, cot_all.T)
    gu_grad, down_grad, mix_got, d_got, gain_total = reduce(
        n, n_tp, turned, *sides, d_both, hidden_e, gain_row, early_all, gu_all, down_all, late_all
    )
    if turned:
        gate_grad, up_grad, down_grad = gu_grad[:width].T, gu_grad[width:].T, down_grad.T
    else:
        gate_grad, up_grad = gu_grad[:, :width], gu_grad[:, width:]

    def gathered(got):
        total = got[0].astype(jnp.float32)
        for k in range(1, n_tp):
            total = total + got[k].astype(jnp.float32)
        return total

    values = late_input.astype(jnp.float32)
    values_e = early_input.astype(jnp.float32)
    scale_e = lax.rsqrt(jnp.mean(values_e * values_e, axis=-1, keepdims=True) + epsilon)
    late_out = (values + 0.5 * gathered(mix_got)).astype(jnp.bfloat16)
    scaled_grad = gathered(d_got) * gain_f
    early_grad = (
        cotangent.astype(jnp.float32)
        + scale_e * scaled_grad
        - values_e * scale_e**3 * jnp.mean(values_e * scaled_grad, axis=-1, keepdims=True)
    ).astype(jnp.bfloat16)
    return (
        late_out,
        early_grad,
        gate_sum + gate_grad,
        up_sum + up_grad,
        down_sum + down_grad,
        gain_sum + gain_total.reshape(depth),
    )


def solution(mesh):
    token = P(("fs", "tp"), None)
    weight = P("fs", "tp")
    return jax.shard_map(
        functools.partial(per_device, mesh.shape["fs"], mesh.shape["tp"]),
        mesh=mesh,
        in_specs=(token, P(), weight, weight, weight, token, token, weight, weight, weight, P()),
        out_specs=(token, token, weight, weight, weight, P()),
        check_vma=False,
    )
```

```python
import functools

import jax
import jax.numpy as jnp
from jax import lax
from jax.experimental import pallas as pl
from jax.experimental.pallas import tpu as pltpu
from jax.sharding import PartitionSpec as P

epsilon = 1e-05
MESH = pl.DeviceIdType.MESH
VMEM_LIMIT = 60 * 1024 * 1024


def ring_place(index, n):
    odd = lax.rem(index, 2)
    half = index // 2
    return (1 - odd) * half + odd * (n - 1 - half)


def ring_index(place, n):
    back = place // (n // 2)
    return (1 - back) * (2 * place) + back * (2 * (n - 1 - place) + 1)


def neighbours(n):
    place = ring_place(lax.axis_index("fs"), n)
    right = ring_index(lax.rem(place + 1, n), n)
    left = ring_index(lax.rem(place + n - 1, n), n)
    return place, right, left


def greet(n_tp, right, left):
    me_tp = lax.axis_index("tp")
    barrier = pltpu.get_barrier_semaphore()
    for target in (right, left):
        pl.semaphore_signal(barrier, inc=1, device_id=(target, me_tp), device_id_type=MESH)
    for away in range(1, n_tp):
        peer = lax.rem(me_tp + away, n_tp)
        pl.semaphore_signal(
            barrier, inc=1, device_id=(lax.axis_index("fs"), peer), device_id_type=MESH
        )
    pl.semaphore_wait(barrier, 2 + n_tp - 1)


def gather_kernel(n, n_tp, turned, *refs):
    gate_in, up_in, dn_in, late_in, early_in, cot_ref, gain_ref = refs[:7]
    gu_out, dn_out, late_all, early_out, cot_out, both_out, hid_out = refs[7:14]
    gate_buf, up_buf, gu_ref, dn_buf, dn_ref, late_buf, early_buf, late_ref = refs[14:22]
    gu_all, dn_all, early_all, cot_all, sum_gu, sum_dn = refs[22:28]
    send_sem, recv_sem, tp_send, tp_recv, own_sem, in_sem, out_sem = refs[28:]
    me_fs, me_tp = lax.axis_index("fs"), lax.axis_index("tp")
    tokens = late_in.shape[0]
    mine = pl.ds(pl.multiple_of(me_tp * tokens, tokens), tokens)
    rows, width = dn_ref.shape
    loads = [
        pltpu.make_async_copy(source, target, in_sem.at[k])
        for k, (source, target) in enumerate(
            (
                (gate_in, gate_buf),
                (up_in, up_buf),
                (early_in, early_buf),
                (late_in, late_buf),
                (dn_in, dn_buf),
                (cot_ref, cot_all.at[mine]),
            )
        )
    ]
    for copy in loads:
        copy.start()
    place, right, left = neighbours(n)
    greet(n_tp, right, left)
    half = rows // 2
    outs = (gu_out, dn_out)
    pairs = ((gu_ref, gu_all), (dn_ref, dn_all))

    def window(owner, way):
        return pl.ds(pl.multiple_of(owner * rows + way * half, half), half)

    def piece(step, c, way, first):
        block, whole = pairs[c]
        if way == 0:
            owner = ring_index(lax.rem(place - step + n, n), n)
            target = right
        else:
            owner = ring_index(lax.rem(place + step, n), n)
            target = left
        spot = whole.at[window(owner, way)]
        source = block.at[pl.ds(way * half, half)] if first else spot
        return pltpu.make_async_remote_copy(
            src_ref=source,
            dst_ref=spot,
            send_sem=send_sem.at[step, c, way],
            recv_sem=recv_sem.at[step, c, way],
            device_id=(target, me_tp),
            device_id_type=MESH,
        )

    token_pairs = (
        (early_all.at[mine], early_all),
        (cot_ref, cot_all),
        (late_ref, late_all),
    )

    def token_piece(a, away):
        block, whole = token_pairs[a]
        return pltpu.make_async_remote_copy(
            src_ref=block,
            dst_ref=whole.at[mine],
            send_sem=tp_send.at[a, away - 1],
            recv_sem=tp_recv.at[a, away - 1],
            device_id=(me_fs, lax.rem(me_tp + away, n_tp)),
            device_id_type=MESH,
        )

    def spread(a):
        for away in range(1, n_tp):
            token_piece(a, away).start()

    def arrived(a):
        for away in range(1, n_tp):
            token_piece(a, away).wait()

    def owner_of(step, way):
        if way == 0:
            return ring_index(lax.rem(place - step + n, n), n)
        return ring_index(lax.rem(place + step, n), n)

    def landed(step, c, way):
        some = window(owner_of(step + 1, way), way)
        return pltpu.make_async_copy(
            pairs[c][1].at[some], outs[c].at[some], out_sem.at[step, c, way]
        )

    totals = ((sum_gu, early_all), (sum_dn, cot_all))

    def add_rows(step, c):
        total, left = totals[c]
        for way in range(2):
            some = window(owner_of(step, way), way)
            total[...] += jnp.dot(
                left[:, some], pairs[c][1][some, :], preferred_element_type=jnp.float32
            )

    def norm(source, target, base):
        def part(k, carry):
            some = pl.ds(pl.multiple_of(k * 16, 16), 16)
            values = source[some, :].astype(jnp.float32)
            scale = lax.rsqrt(jnp.mean(values * values, axis=-1, keepdims=True) + epsilon)
            target[pl.ds(pl.multiple_of(base + k * 16, 16), 16), :] = (values * scale * gain_ref[...]).astype(jnp.bfloat16)
            return carry

        lax.fori_loop(0, tokens // 16, part, 0)

    def plain(buffer):
        return buffer[...].T if turned else buffer[...]

    loads[4].wait()
    dn_ref[...] = plain(dn_buf)
    for way in range(2):
        piece(0, 1, way, True).start()
    loads[0].wait()
    loads[1].wait()
    gu_ref[:, :width] = plain(gate_buf)
    gu_ref[:, width:] = plain(up_buf)
    for way in range(2):
        piece(0, 0, way, True).start()
    loads[2].wait()
    norm(early_buf, early_all, me_tp * tokens)
    spread(0)
    spread(1)
    loads[3].wait()
    norm(late_buf, late_ref, 0)
    spread(2)
    loads[5].wait()
    here = pl.ds(pl.multiple_of(me_fs * rows, rows), rows)
    gu_all[here, :] = gu_ref[...]
    dn_all[here, :] = dn_ref[...]
    sum_gu[...] = jnp.zeros_like(sum_gu)
    sum_dn[...] = jnp.zeros_like(sum_dn)
    own = [
        pltpu.make_async_copy(late_ref, late_all.at[mine], own_sem.at[0]),
        pltpu.make_async_copy(gu_ref, gu_out.at[here], own_sem.at[1]),
        pltpu.make_async_copy(dn_ref, dn_out.at[here], own_sem.at[2]),
    ]
    for copy in own:
        copy.start()
    keep = [
        pltpu.make_async_copy(early_all, early_out, own_sem.at[3]),
        pltpu.make_async_copy(cot_all, cot_out, own_sem.at[4]),
    ]

    def body(step, carry):
        for c in (1, 0):
            for way in range(2):
                piece(step - 1, c, way, False).wait_recv()
                piece(step, c, way, False).start()
                landed(step - 1, c, way).start()
            which = 1 - c

            @pl.when(step == n // 2)
            def _():
                arrived(which)
                keep[which].start()

            if turned:

                @pl.when(step >= n // 2)
                def _():
                    add_rows(2 * (step - n // 2), which)
                    add_rows(2 * (step - n // 2) + 1, which)

        return carry

    lax.fori_loop(1, n - 1, body, 0)
    if turned:
        for c in (1, 0):
            add_rows(n - 2, c)
    for c in (1, 0):
        for way in range(2):
            piece(n - 2, c, way, False).wait_recv()
            landed(n - 2, c, way).start()
            piece(0, c, way, True).wait_send()
        if turned:
            add_rows(n - 1, c)
        else:
            total, rest = totals[c]
            total[...] = jnp.dot(
                rest[...], pairs[c][1][...], preferred_element_type=jnp.float32
            )

    def finish(k, carry):
        some = pl.ds(pl.multiple_of(k * 16, 16), 16)
        gate, upper = sum_gu[some, :width], sum_gu[some, width:]
        sigma = 1.0 / (1.0 + jnp.exp(-gate))
        d_hidden = 0.5 * sum_dn[some, :]
        hid_out[some, :] = (gate * sigma * upper).astype(jnp.bfloat16)
        both_out[some, :width] = (
            d_hidden * upper * sigma * (1.0 + gate * (1.0 - sigma))
        ).astype(jnp.bfloat16)
        both_out[some, width:] = (d_hidden * gate * sigma).astype(jnp.bfloat16)
        return carry

    lax.fori_loop(0, n_tp * tokens // 16, finish, 0)

    def drain(step, carry):
        for c in (1, 0):
            for way in range(2):
                piece(step, c, way, False).wait_send()
        return carry

    lax.fori_loop(1, n - 1, drain, 0)

    def put(step, carry):
        for c in range(2):
            for way in range(2):
                landed(step, c, way).wait()
        return carry

    lax.fori_loop(0, n - 1, put, 0)
    for copy in own + keep:
        copy.wait()
    arrived(2)


def gather(n, n_tp, turned, gate, up, dn, late, early, cot, gain):
    rows, width = gate.shape[::-1] if turned else gate.shape
    tokens, depth = late.shape
    vmem = pl.BlockSpec(memory_space=pltpu.VMEM)
    hbm = pl.BlockSpec(memory_space=pl.ANY)
    bf16 = jnp.bfloat16
    return pl.pallas_call(
        functools.partial(gather_kernel, n, n_tp, turned),
        out_shape=[
            jax.ShapeDtypeStruct((n * rows, 2 * width), bf16),
            jax.ShapeDtypeStruct((n * rows, width), bf16),
        ]
        + [jax.ShapeDtypeStruct((n_tp * tokens, depth), bf16)] * 3
        + [
            jax.ShapeDtypeStruct((n_tp * tokens, 2 * width), bf16),
            jax.ShapeDtypeStruct((n_tp * tokens, width), bf16),
        ],
        in_specs=[hbm] * 6 + [vmem],
        out_specs=[hbm] * 5 + [vmem] * 2,
        scratch_shapes=[
            pltpu.VMEM(gate.shape, bf16),
            pltpu.VMEM(gate.shape, bf16),
            pltpu.VMEM((rows, 2 * width), bf16),
            pltpu.VMEM(gate.shape, bf16),
            pltpu.VMEM((rows, width), bf16),
        ]
        + [pltpu.VMEM((tokens, depth), bf16)] * 3
        + [
            pltpu.VMEM((n * rows, 2 * width), bf16),
            pltpu.VMEM((n * rows, width), bf16),
            pltpu.VMEM((n_tp * tokens, depth), bf16),
            pltpu.VMEM((n_tp * tokens, depth), bf16),
            pltpu.VMEM((n_tp * tokens, 2 * width), jnp.float32),
            pltpu.VMEM((n_tp * tokens, width), jnp.float32),
        ]
        + [
            pltpu.SemaphoreType.DMA((n - 1, 2, 2)),
            pltpu.SemaphoreType.DMA((n - 1, 2, 2)),
            pltpu.SemaphoreType.DMA((3, n_tp - 1)),
            pltpu.SemaphoreType.DMA((3, n_tp - 1)),
            pltpu.SemaphoreType.DMA((5,)),
            pltpu.SemaphoreType.DMA((6,)),
            pltpu.SemaphoreType.DMA((n - 1, 2, 2)),
        ],
        compiler_params=pltpu.CompilerParams(
            collective_id=0, has_side_effects=True, vmem_limit_bytes=VMEM_LIMIT
        ),
    )(gate, up, dn, late, early, cot, gain)


def reduce_kernel(n, n_tp, turned, *refs):
    early_side, cot_side, both_ref, hid_ref, gain_ref, early_all, gu_in, dn_in, late_in = refs[:9]
    gu_out, dn_out, mix_out, dnorm_out, gain_out = refs[9:14]
    gu_slots, dn_slots, gain_slots, gain_tp, gu_first, dn_first = refs[14:20]
    gu_all, dn_all, late_all, mix_ref, dnorm_ref, gain_sum = refs[20:26]
    send_sem, recv_sem, gain_send, gain_recv, tp_send, tp_recv, last_send, last_recv = refs[26:34]
    in_sem, own_sem = refs[34:]
    loads = [
        pltpu.make_async_copy(source, target, in_sem.at[k])
        for k, (source, target) in enumerate(
            ((gu_in, gu_all), (late_in, late_all), (dn_in, dn_all))
        )
    ]
    for copy in loads:
        copy.start()
    me_fs, me_tp = lax.axis_index("fs"), lax.axis_index("tp")
    place, right, left = neighbours(n)
    barrier = pltpu.get_barrier_semaphore()

    def greet_fs(away, carry):
        target = lax.rem(me_fs + away, n)
        pl.semaphore_signal(barrier, inc=1, device_id=(target, me_tp), device_id_type=MESH)
        return carry

    lax.fori_loop(1, n, greet_fs, 0)
    for away in range(1, n_tp):
        peer = lax.rem(me_tp + away, n_tp)
        pl.semaphore_signal(barrier, inc=1, device_id=(me_fs, peer), device_id_type=MESH)
    pl.semaphore_wait(barrier, n - 1 + n_tp - 1)
    width = dn_all.shape[1]
    half = gu_first.shape[1]
    rows = 2 * half
    tokens = late_all.shape[0] // n_tp
    sets = ((gu_first, gu_slots), (dn_first, dn_slots))
    factors = ((early_side, both_ref, 1.0), (cot_side, hid_ref, 0.5))

    def local(step, way):
        if way == 0:
            owner = ring_index(lax.rem(place - step - 1 + n, n), n)
        else:
            owner = ring_index(lax.rem(place + step + 1, n), n)
        return pl.ds(pl.multiple_of(owner * rows + way * half, half), half)

    def product(step, c, way):
        side, other, factor = factors[c]
        if turned:
            left, contract = side[:, local(step, way)], 0
        else:
            left, contract = side[local(step, way), :], 1
        return factor * lax.dot_general(
            left,
            other[...],
            (((contract,), (0,)), ((), ())),
            preferred_element_type=jnp.float32,
        )

    def piece(step, c, way, first, landed=False):
        start, slots = sets[c]
        source = start.at[way] if first else slots.at[way, step if landed else step - 1]
        return pltpu.make_async_remote_copy(
            src_ref=source,
            dst_ref=slots.at[way, step],
            send_sem=send_sem.at[step, c, way],
            recv_sem=recv_sem.at[step, c, way],
            device_id=((left if way else right), me_tp),
            device_id_type=MESH,
        )

    def gain_piece(away):
        return pltpu.make_async_remote_copy(
            src_ref=gain_slots.at[me_fs],
            dst_ref=gain_slots.at[me_fs],
            send_sem=gain_send.at[away - 1],
            recv_sem=gain_recv.at[away - 1],
            device_id=(lax.rem(me_fs + away, n), me_tp),
            device_id_type=MESH,
        )

    results = ((dnorm_ref, dnorm_out), (mix_ref, mix_out))

    def share(a, away):
        source, target = results[a]
        return pltpu.make_async_remote_copy(
            src_ref=source.at[away - 1],
            dst_ref=target.at[away - 1],
            send_sem=tp_send.at[a, away - 1],
            recv_sem=tp_recv.at[a, away - 1],
            device_id=(me_fs, lax.rem(me_tp + away, n_tp)),
            device_id_type=MESH,
        )

    def keep(a):
        source, target = results[a]
        return pltpu.make_async_copy(source.at[n_tp - 1], target.at[n_tp - 1], own_sem.at[a])

    def block_of(away):
        return pl.ds(pl.multiple_of(lax.rem(me_tp + away, n_tp) * tokens, tokens), tokens)

    def grad_block(away):
        some = block_of(away)
        part = lax.dot_general(
            both_ref[some, :],
            gu_all[...],
            (((1,), (1,)), ((), ())),
            preferred_element_type=jnp.float32,
        ).astype(jnp.bfloat16)
        dnorm_ref[away - 1] = part
        gain_sum[...] += jnp.sum(
            part.astype(jnp.float32) * early_all[some, :].astype(jnp.float32),
            axis=0,
            keepdims=True,
        )

    def late_block(away):
        both = jnp.dot(
            late_all[block_of(away), :], gu_all[...], preferred_element_type=jnp.float32
        )
        gate = both[:, :width]
        hidden = (gate / (1.0 + jnp.exp(-gate)) * both[:, width:]).astype(jnp.bfloat16)
        mix_ref[away - 1] = lax.dot_general(
            hidden, dn_all[...], (((1,), (1,)), ((), ())), preferred_element_type=jnp.float32
        ).astype(jnp.bfloat16)

    for c in range(2):
        for way in range(2):
            sets[c][0][way] = product(0, c, way).astype(jnp.bfloat16)
            piece(0, c, way, True).start()
    gain_sum[...] = jnp.zeros_like(gain_sum)
    for copy in loads:
        copy.wait()

    for c in range(2):
        (grad_block, late_block)[c](1)
        share(c, 1).start()

    def body(step, carry):
        for c in range(2):
            slots = sets[c][1]
            for way in range(2):
                term = product(step, c, way)
                piece(step - 1, c, way, False, True).wait_recv()
                slots[way, step - 1] = (
                    slots[way, step - 1].astype(jnp.float32) + term
                ).astype(jnp.bfloat16)
                piece(step, c, way, False).start()

            @pl.when(step < n_tp)
            def _():
                (grad_block, late_block)[c](step + 1)

            @pl.when(step < n_tp - 1)
            def _():
                share(c, step + 1).start()

            @pl.when(step == n_tp - 1)
            def _():
                keep(c).start()

        @pl.when(step == n_tp - 1)
        def _():
            gain_slots[me_fs] = gain_sum[...] / gain_ref[...]

            def send(away, inner):
                gain_piece(away).start()
                return inner

            lax.fori_loop(1, n, send, 0)

        return carry

    lax.fori_loop(1, n - 1, body, 0)

    def settle(away, inner):
        gain_piece(away).wait()
        return inner

    lax.fori_loop(1, n, settle, 0)
    gain_tp[me_tp] = lax.fori_loop(
        1, n, lambda k, total: total + gain_slots[k], gain_slots[0]
    )
    last = []
    for away in range(1, n_tp):
        peer = lax.rem(me_tp + away, n_tp)
        copy = pltpu.make_async_remote_copy(
            src_ref=gain_tp.at[me_tp],
            dst_ref=gain_tp.at[me_tp],
            send_sem=last_send.at[away - 1],
            recv_sem=last_recv.at[away - 1],
            device_id=(me_fs, peer),
            device_id_type=MESH,
        )
        copy.start()
        last.append(copy)
    for c in range(2):
        slots = sets[c][1]
        for way in range(2):
            term = product(n - 1, c, way)
            piece(n - 2, c, way, False, True).wait_recv()
            total = slots[way, n - 2].astype(jnp.float32) + term
            out = (gu_out, dn_out)[c]
            if turned:
                out[:, pl.ds(way * half, half)] = total.T
            else:
                out[pl.ds(way * half, half), :] = total
            piece(0, c, way, True).wait_send()
    for copy in last:
        copy.wait()
    total = gain_tp[0]
    for k in range(1, n_tp):
        total = total + gain_tp[k]
    gain_out[...] = total

    def drain(step, carry):
        for c in range(2):
            for way in range(2):
                piece(step, c, way, False).wait_send()
        return carry

    lax.fori_loop(1, n - 1, drain, 0)
    for a in range(2):
        keep(a).wait()
        for away in range(1, n_tp):
            share(a, away).wait()


def reduce(n, n_tp, turned, early_side, cot_side, both, hid, gain, early_all, gu_all, dn_all, late_all):
    rows = gu_all.shape[0] // n
    half = rows // 2
    width = dn_all.shape[1]
    shapes = [(rows, 2 * width), (rows, width)]
    if turned:
        shapes = [shape[::-1] for shape in shapes]
    depth = late_all.shape[1]
    tokens = late_all.shape[0] // n_tp
    vmem = pl.BlockSpec(memory_space=pltpu.VMEM)
    hbm = pl.BlockSpec(memory_space=pl.ANY)
    f32, bf16 = jnp.float32, jnp.bfloat16
    return pl.pallas_call(
        functools.partial(reduce_kernel, n, n_tp, turned),
        out_shape=[
            jax.ShapeDtypeStruct(shapes[0], f32),
            jax.ShapeDtypeStruct(shapes[1], f32),
            jax.ShapeDtypeStruct((n_tp, tokens, depth), bf16),
            jax.ShapeDtypeStruct((n_tp, tokens, depth), bf16),
            jax.ShapeDtypeStruct(gain.shape, f32),
        ],
        in_specs=[vmem] * 6 + [hbm] * 3,
        out_specs=[vmem, vmem, hbm, hbm, vmem],
        scratch_shapes=[
            pltpu.VMEM((2, n - 1, half, 2 * width), bf16),
            pltpu.VMEM((2, n - 1, half, width), bf16),
            pltpu.VMEM((n,) + gain.shape, f32),
            pltpu.VMEM((n_tp,) + gain.shape, f32),
            pltpu.VMEM((2, half, 2 * width), bf16),
            pltpu.VMEM((2, half, width), bf16),
            pltpu.VMEM(gu_all.shape, bf16),
            pltpu.VMEM(dn_all.shape, bf16),
            pltpu.VMEM(late_all.shape, bf16),
            pltpu.VMEM((n_tp, tokens, depth), bf16),
            pltpu.VMEM((n_tp, tokens, depth), bf16),
            pltpu.VMEM(gain.shape, f32),
            pltpu.SemaphoreType.DMA((n - 1, 2, 2)),
            pltpu.SemaphoreType.DMA((n - 1, 2, 2)),
            pltpu.SemaphoreType.DMA((n - 1,)),
            pltpu.SemaphoreType.DMA((n - 1,)),
            pltpu.SemaphoreType.DMA((2, n_tp - 1)),
            pltpu.SemaphoreType.DMA((2, n_tp - 1)),
            pltpu.SemaphoreType.DMA((n_tp - 1,)),
            pltpu.SemaphoreType.DMA((n_tp - 1,)),
            pltpu.SemaphoreType.DMA((3,)),
            pltpu.SemaphoreType.DMA((2,)),
        ],
        compiler_params=pltpu.CompilerParams(
            collective_id=1, has_side_effects=True, vmem_limit_bytes=VMEM_LIMIT
        ),
    )(early_side, cot_side, both, hid, gain, early_all, gu_all, dn_all, late_all)


def per_device(
    n,
    n_tp,
    late_input,
    norm_gain,
    gate_weight,
    up_weight,
    down_weight,
    early_input,
    cotangent,
    gate_sum,
    up_sum,
    down_sum,
    gain_sum,
):
    gain_f = norm_gain.astype(jnp.float32)
    width = gate_weight.shape[1]
    depth = late_input.shape[1]
    turned = gate_weight.shape[0] % 256 == 0
    weights = [gate_weight, up_weight, down_weight]
    if turned:
        weights = [weight.T for weight in weights]
    gain_row = gain_f.reshape(1, depth)
    gu_all, down_all, late_all, early_all, cot_all, d_both, hidden_e = gather(
        n, n_tp, turned, *weights, late_input, early_input, cotangent, gain_row
    )
    sides = (early_all, cot_all) if turned else (early_all.T, cot_all.T)
    gu_grad, down_grad, mix_got, d_got, gain_total = reduce(
        n, n_tp, turned, *sides, d_both, hidden_e, gain_row, early_all, gu_all, down_all, late_all
    )
    if turned:
        gate_grad, up_grad, down_grad = gu_grad[:width].T, gu_grad[width:].T, down_grad.T
    else:
        gate_grad, up_grad = gu_grad[:, :width], gu_grad[:, width:]

    def gathered(got):
        total = got[0].astype(jnp.float32)
        for k in range(1, n_tp):
            total = total + got[k].astype(jnp.float32)
        return total

    values = late_input.astype(jnp.float32)
    values_e = early_input.astype(jnp.float32)
    scale_e = lax.rsqrt(jnp.mean(values_e * values_e, axis=-1, keepdims=True) + epsilon)
    late_out = (values + 0.5 * gathered(mix_got)).astype(jnp.bfloat16)
    scaled_grad = gathered(d_got) * gain_f
    early_grad = (
        cotangent.astype(jnp.float32)
        + scale_e * scaled_grad
        - values_e * scale_e**3 * jnp.mean(values_e * scaled_grad, axis=-1, keepdims=True)
    ).astype(jnp.bfloat16)
    return (
        late_out,
        early_grad,
        gate_sum + gate_grad,
        up_sum + up_grad,
        down_sum + down_grad,
        gain_sum + gain_total.reshape(depth),
    )


def solution(mesh):
    token = P(("fs", "tp"), None)
    weight = P("fs", "tp")
    return jax.shard_map(
        functools.partial(per_device, mesh.shape["fs"], mesh.shape["tp"]),
        mesh=mesh,
        in_specs=(token, P(), weight, weight, weight, token, token, weight, weight, weight, P()),
        out_specs=(token, token, weight, weight, weight, P()),
        check_vma=False,
    )
```

```python
import functools

import jax
import jax.numpy as jnp
from jax import lax
from jax.experimental import pallas as pl
from jax.experimental.pallas import tpu as pltpu
from jax.sharding import PartitionSpec as P

epsilon = 1e-05
MESH = pl.DeviceIdType.MESH
VMEM_LIMIT = 60 * 1024 * 1024


def ring_place(index, n):
    odd = lax.rem(index, 2)
    half = index // 2
    return (1 - odd) * half + odd * (n - 1 - half)


def ring_index(place, n):
    back = place // (n // 2)
    return (1 - back) * (2 * place) + back * (2 * (n - 1 - place) + 1)


def neighbours(n):
    place = ring_place(lax.axis_index("fs"), n)
    right = ring_index(lax.rem(place + 1, n), n)
    left = ring_index(lax.rem(place + n - 1, n), n)
    return place, right, left


def greet(n_tp, right, left):
    me_tp = lax.axis_index("tp")
    barrier = pltpu.get_barrier_semaphore()
    for target in (right, left):
        pl.semaphore_signal(barrier, inc=1, device_id=(target, me_tp), device_id_type=MESH)
    for away in range(1, n_tp):
        peer = lax.rem(me_tp + away, n_tp)
        pl.semaphore_signal(
            barrier, inc=1, device_id=(lax.axis_index("fs"), peer), device_id_type=MESH
        )
    pl.semaphore_wait(barrier, 2 + n_tp - 1)


def gather_kernel(n, n_tp, turned, *refs):
    gate_in, up_in, dn_in, late_in, early_in, cot_ref, gain_ref = refs[:7]
    gu_out, dn_out, late_all, early_out, cot_out, both_out, hid_out = refs[7:14]
    gate_buf, up_buf, gu_ref, dn_buf, dn_ref, late_buf, early_buf, late_ref = refs[14:22]
    gu_all, dn_all, early_all, cot_all, sum_gu, sum_dn = refs[22:28]
    send_sem, recv_sem, tp_send, tp_recv, own_sem, in_sem, out_sem = refs[28:]
    me_fs, me_tp = lax.axis_index("fs"), lax.axis_index("tp")
    tokens = late_in.shape[0]
    mine = pl.ds(pl.multiple_of(me_tp * tokens, tokens), tokens)
    rows, width = dn_ref.shape
    loads = [
        pltpu.make_async_copy(source, target, in_sem.at[k])
        for k, (source, target) in enumerate(
            (
                (gate_in, gate_buf),
                (up_in, up_buf),
                (early_in, early_buf),
                (late_in, late_buf),
                (dn_in, dn_buf),
                (cot_ref, cot_all.at[mine]),
            )
        )
    ]
    for copy in loads:
        copy.start()
    place, right, left = neighbours(n)
    greet(n_tp, right, left)
    half = rows // 2
    outs = (gu_out, dn_out)
    pairs = ((gu_ref, gu_all), (dn_ref, dn_all))

    def window(owner, way):
        return pl.ds(pl.multiple_of(owner * rows + way * half, half), half)

    def piece(step, c, way, first):
        block, whole = pairs[c]
        if way == 0:
            owner = ring_index(lax.rem(place - step + n, n), n)
            target = right
        else:
            owner = ring_index(lax.rem(place + step, n), n)
            target = left
        spot = whole.at[window(owner, way)]
        source = block.at[pl.ds(way * half, half)] if first else spot
        return pltpu.make_async_remote_copy(
            src_ref=source,
            dst_ref=spot,
            send_sem=send_sem.at[step, c, way],
            recv_sem=recv_sem.at[step, c, way],
            device_id=(target, me_tp),
            device_id_type=MESH,
        )

    token_pairs = (
        (early_all.at[mine], early_all),
        (cot_ref, cot_all),
        (late_ref, late_all),
    )

    def token_piece(a, away):
        block, whole = token_pairs[a]
        return pltpu.make_async_remote_copy(
            src_ref=block,
            dst_ref=whole.at[mine],
            send_sem=tp_send.at[a, away - 1],
            recv_sem=tp_recv.at[a, away - 1],
            device_id=(me_fs, lax.rem(me_tp + away, n_tp)),
            device_id_type=MESH,
        )

    def spread(a):
        for away in range(1, n_tp):
            token_piece(a, away).start()

    def arrived(a):
        for away in range(1, n_tp):
            token_piece(a, away).wait()

    def owner_of(step, way):
        if way == 0:
            return ring_index(lax.rem(place - step + n, n), n)
        return ring_index(lax.rem(place + step, n), n)

    def landed(step, c, way):
        some = window(owner_of(step + 1, way), way)
        return pltpu.make_async_copy(
            pairs[c][1].at[some], outs[c].at[some], out_sem.at[step, c, way]
        )

    totals = ((sum_gu, early_all), (sum_dn, cot_all))

    def add_rows(step, c):
        total, left = totals[c]
        for way in range(2):
            some = window(owner_of(step, way), way)
            total[...] += jnp.dot(
                left[:, some], pairs[c][1][some, :], preferred_element_type=jnp.float32
            )

    def norm(source, target, base):
        def part(k, carry):
            some = pl.ds(pl.multiple_of(k * 16, 16), 16)
            values = source[some, :].astype(jnp.float32)
            scale = lax.rsqrt(jnp.mean(values * values, axis=-1, keepdims=True) + epsilon)
            target[pl.ds(pl.multiple_of(base + k * 16, 16), 16), :] = (values * scale * gain_ref[...]).astype(jnp.bfloat16)
            return carry

        lax.fori_loop(0, tokens // 16, part, 0)

    def plain(buffer):
        return buffer[...].T if turned else buffer[...]

    loads[4].wait()
    dn_ref[...] = plain(dn_buf)
    for way in range(2):
        piece(0, 1, way, True).start()
    loads[0].wait()
    loads[1].wait()
    gu_ref[:, :width] = plain(gate_buf)
    gu_ref[:, width:] = plain(up_buf)
    for way in range(2):
        piece(0, 0, way, True).start()
    loads[2].wait()
    norm(early_buf, early_all, me_tp * tokens)
    spread(0)
    spread(1)
    loads[3].wait()
    norm(late_buf, late_ref, 0)
    spread(2)
    loads[5].wait()
    here = pl.ds(pl.multiple_of(me_fs * rows, rows), rows)
    gu_all[here, :] = gu_ref[...]
    dn_all[here, :] = dn_ref[...]
    sum_gu[...] = jnp.zeros_like(sum_gu)
    sum_dn[...] = jnp.zeros_like(sum_dn)
    own = [
        pltpu.make_async_copy(late_ref, late_all.at[mine], own_sem.at[0]),
        pltpu.make_async_copy(gu_ref, gu_out.at[here], own_sem.at[1]),
        pltpu.make_async_copy(dn_ref, dn_out.at[here], own_sem.at[2]),
    ]
    for copy in own:
        copy.start()
    keep = [
        pltpu.make_async_copy(early_all, early_out, own_sem.at[3]),
        pltpu.make_async_copy(cot_all, cot_out, own_sem.at[4]),
    ]

    def body(step, carry):
        for c in (1, 0):
            for way in range(2):
                piece(step - 1, c, way, False).wait_recv()
                piece(step, c, way, False).start()
                landed(step - 1, c, way).start()
            which = 1 - c

            @pl.when(step == n // 2)
            def _():
                arrived(which)
                keep[which].start()

            if turned:

                @pl.when(step >= n // 2)
                def _():
                    add_rows(2 * (step - n // 2), which)
                    add_rows(2 * (step - n // 2) + 1, which)

        return carry

    lax.fori_loop(1, n - 1, body, 0)
    if turned:
        for c in (1, 0):
            add_rows(n - 2, c)
    for c in (1, 0):
        for way in range(2):
            piece(n - 2, c, way, False).wait_recv()
            landed(n - 2, c, way).start()
            piece(0, c, way, True).wait_send()
        if turned:
            add_rows(n - 1, c)
        else:
            total, rest = totals[c]
            total[...] = jnp.dot(
                rest[...], pairs[c][1][...], preferred_element_type=jnp.float32
            )

    def finish(k, carry):
        some = pl.ds(pl.multiple_of(k * 64, 64), 64)
        gate, upper = sum_gu[some, :width], sum_gu[some, width:]
        sigma = 1.0 / (1.0 + jnp.exp(-gate))
        d_hidden = 0.5 * sum_dn[some, :]
        hid_out[some, :] = (gate * sigma * upper).astype(jnp.bfloat16)
        both_out[some, :width] = (
            d_hidden * upper * sigma * (1.0 + gate * (1.0 - sigma))
        ).astype(jnp.bfloat16)
        both_out[some, width:] = (d_hidden * gate * sigma).astype(jnp.bfloat16)
        return carry

    lax.fori_loop(0, n_tp * tokens // 64, finish, 0)

    def drain(step, carry):
        for c in (1, 0):
            for way in range(2):
                piece(step, c, way, False).wait_send()
        return carry

    lax.fori_loop(1, n - 1, drain, 0)

    def put(step, carry):
        for c in range(2):
            for way in range(2):
                landed(step, c, way).wait()
        return carry

    lax.fori_loop(0, n - 1, put, 0)
    for copy in own + keep:
        copy.wait()
    arrived(2)


def gather(n, n_tp, turned, gate, up, dn, late, early, cot, gain):
    rows, width = gate.shape[::-1] if turned else gate.shape
    tokens, depth = late.shape
    vmem = pl.BlockSpec(memory_space=pltpu.VMEM)
    hbm = pl.BlockSpec(memory_space=pl.ANY)
    bf16 = jnp.bfloat16
    return pl.pallas_call(
        functools.partial(gather_kernel, n, n_tp, turned),
        out_shape=[
            jax.ShapeDtypeStruct((n * rows, 2 * width), bf16),
            jax.ShapeDtypeStruct((n * rows, width), bf16),
        ]
        + [jax.ShapeDtypeStruct((n_tp * tokens, depth), bf16)] * 3
        + [
            jax.ShapeDtypeStruct((n_tp * tokens, 2 * width), bf16),
            jax.ShapeDtypeStruct((n_tp * tokens, width), bf16),
        ],
        in_specs=[hbm] * 6 + [vmem],
        out_specs=[hbm] * 5 + [vmem] * 2,
        scratch_shapes=[
            pltpu.VMEM(gate.shape, bf16),
            pltpu.VMEM(gate.shape, bf16),
            pltpu.VMEM((rows, 2 * width), bf16),
            pltpu.VMEM(gate.shape, bf16),
            pltpu.VMEM((rows, width), bf16),
        ]
        + [pltpu.VMEM((tokens, depth), bf16)] * 3
        + [
            pltpu.VMEM((n * rows, 2 * width), bf16),
            pltpu.VMEM((n * rows, width), bf16),
            pltpu.VMEM((n_tp * tokens, depth), bf16),
            pltpu.VMEM((n_tp * tokens, depth), bf16),
            pltpu.VMEM((n_tp * tokens, 2 * width), jnp.float32),
            pltpu.VMEM((n_tp * tokens, width), jnp.float32),
        ]
        + [
            pltpu.SemaphoreType.DMA((n - 1, 2, 2)),
            pltpu.SemaphoreType.DMA((n - 1, 2, 2)),
            pltpu.SemaphoreType.DMA((3, n_tp - 1)),
            pltpu.SemaphoreType.DMA((3, n_tp - 1)),
            pltpu.SemaphoreType.DMA((5,)),
            pltpu.SemaphoreType.DMA((6,)),
            pltpu.SemaphoreType.DMA((n - 1, 2, 2)),
        ],
        compiler_params=pltpu.CompilerParams(
            collective_id=0, has_side_effects=True, vmem_limit_bytes=VMEM_LIMIT
        ),
    )(gate, up, dn, late, early, cot, gain)


def reduce_kernel(n, n_tp, turned, *refs):
    early_side, cot_side, both_ref, hid_ref, gain_ref, early_all, gu_in, dn_in, late_in = refs[:9]
    gu_out, dn_out, mix_out, dnorm_out, gain_out = refs[9:14]
    gu_slots, dn_slots, gain_slots, gain_tp, gu_first, dn_first = refs[14:20]
    gu_all, dn_all, late_all, mix_ref, dnorm_ref, gain_sum = refs[20:26]
    send_sem, recv_sem, gain_send, gain_recv, tp_send, tp_recv, last_send, last_recv = refs[26:34]
    in_sem, own_sem = refs[34:]
    loads = [
        pltpu.make_async_copy(source, target, in_sem.at[k])
        for k, (source, target) in enumerate(
            ((gu_in, gu_all), (late_in, late_all), (dn_in, dn_all))
        )
    ]
    for copy in loads:
        copy.start()
    me_fs, me_tp = lax.axis_index("fs"), lax.axis_index("tp")
    place, right, left = neighbours(n)
    barrier = pltpu.get_barrier_semaphore()

    def greet_fs(away, carry):
        target = lax.rem(me_fs + away, n)
        pl.semaphore_signal(barrier, inc=1, device_id=(target, me_tp), device_id_type=MESH)
        return carry

    lax.fori_loop(1, n, greet_fs, 0)
    for away in range(1, n_tp):
        peer = lax.rem(me_tp + away, n_tp)
        pl.semaphore_signal(barrier, inc=1, device_id=(me_fs, peer), device_id_type=MESH)
    pl.semaphore_wait(barrier, n - 1 + n_tp - 1)
    width = dn_all.shape[1]
    half = gu_first.shape[1]
    rows = 2 * half
    tokens = late_all.shape[0] // n_tp
    sets = ((gu_first, gu_slots), (dn_first, dn_slots))
    factors = ((early_side, both_ref, 1.0), (cot_side, hid_ref, 0.5))

    def local(step, way):
        if way == 0:
            owner = ring_index(lax.rem(place - step - 1 + n, n), n)
        else:
            owner = ring_index(lax.rem(place + step + 1, n), n)
        return pl.ds(pl.multiple_of(owner * rows + way * half, half), half)

    def product(step, c, way):
        side, other, factor = factors[c]
        if turned:
            left, contract = side[:, local(step, way)], 0
        else:
            left, contract = side[local(step, way), :], 1
        return factor * lax.dot_general(
            left,
            other[...],
            (((contract,), (0,)), ((), ())),
            preferred_element_type=jnp.float32,
        )

    def piece(step, c, way, first, landed=False):
        start, slots = sets[c]
        source = start.at[way] if first else slots.at[way, step if landed else step - 1]
        return pltpu.make_async_remote_copy(
            src_ref=source,
            dst_ref=slots.at[way, step],
            send_sem=send_sem.at[step, c, way],
            recv_sem=recv_sem.at[step, c, way],
            device_id=((left if way else right), me_tp),
            device_id_type=MESH,
        )

    def gain_piece(away):
        return pltpu.make_async_remote_copy(
            src_ref=gain_slots.at[me_fs],
            dst_ref=gain_slots.at[me_fs],
            send_sem=gain_send.at[away - 1],
            recv_sem=gain_recv.at[away - 1],
            device_id=(lax.rem(me_fs + away, n), me_tp),
            device_id_type=MESH,
        )

    results = ((dnorm_ref, dnorm_out), (mix_ref, mix_out))

    def share(a, away):
        source, target = results[a]
        return pltpu.make_async_remote_copy(
            src_ref=source.at[away - 1],
            dst_ref=target.at[away - 1],
            send_sem=tp_send.at[a, away - 1],
            recv_sem=tp_recv.at[a, away - 1],
            device_id=(me_fs, lax.rem(me_tp + away, n_tp)),
            device_id_type=MESH,
        )

    def keep(a):
        source, target = results[a]
        return pltpu.make_async_copy(source.at[n_tp - 1], target.at[n_tp - 1], own_sem.at[a])

    def block_of(away):
        return pl.ds(pl.multiple_of(lax.rem(me_tp + away, n_tp) * tokens, tokens), tokens)

    def grad_block(away):
        some = block_of(away)
        part = lax.dot_general(
            both_ref[some, :],
            gu_all[...],
            (((1,), (1,)), ((), ())),
            preferred_element_type=jnp.float32,
        ).astype(jnp.bfloat16)
        dnorm_ref[away - 1] = part
        gain_sum[...] += jnp.sum(
            part.astype(jnp.float32) * early_all[some, :].astype(jnp.float32),
            axis=0,
            keepdims=True,
        )

    def late_block(away):
        both = jnp.dot(
            late_all[block_of(away), :], gu_all[...], preferred_element_type=jnp.float32
        )
        gate = both[:, :width]
        hidden = (gate / (1.0 + jnp.exp(-gate)) * both[:, width:]).astype(jnp.bfloat16)
        mix_ref[away - 1] = lax.dot_general(
            hidden, dn_all[...], (((1,), (1,)), ((), ())), preferred_element_type=jnp.float32
        ).astype(jnp.bfloat16)

    for c in range(2):
        for way in range(2):
            sets[c][0][way] = product(0, c, way).astype(jnp.bfloat16)
            piece(0, c, way, True).start()
    gain_sum[...] = jnp.zeros_like(gain_sum)
    for copy in loads:
        copy.wait()

    for c in range(2):
        (grad_block, late_block)[c](1)
        share(c, 1).start()

    def body(step, carry):
        for c in range(2):
            slots = sets[c][1]
            for way in range(2):
                term = product(step, c, way)
                piece(step - 1, c, way, False, True).wait_recv()
                slots[way, step - 1] = (
                    slots[way, step - 1].astype(jnp.float32) + term
                ).astype(jnp.bfloat16)
                piece(step, c, way, False).start()

            @pl.when(step < n_tp)
            def _():
                (grad_block, late_block)[c](step + 1)

            @pl.when(step < n_tp - 1)
            def _():
                share(c, step + 1).start()

            @pl.when(step == n_tp - 1)
            def _():
                keep(c).start()

        @pl.when(step == n_tp - 1)
        def _():
            gain_slots[me_fs] = gain_sum[...] / gain_ref[...]

            def send(away, inner):
                gain_piece(away).start()
                return inner

            lax.fori_loop(1, n, send, 0)

        return carry

    lax.fori_loop(1, n - 1, body, 0)

    def settle(away, inner):
        gain_piece(away).wait()
        return inner

    lax.fori_loop(1, n, settle, 0)
    gain_tp[me_tp] = lax.fori_loop(
        1, n, lambda k, total: total + gain_slots[k], gain_slots[0]
    )
    last = []
    for away in range(1, n_tp):
        peer = lax.rem(me_tp + away, n_tp)
        copy = pltpu.make_async_remote_copy(
            src_ref=gain_tp.at[me_tp],
            dst_ref=gain_tp.at[me_tp],
            send_sem=last_send.at[away - 1],
            recv_sem=last_recv.at[away - 1],
            device_id=(me_fs, peer),
            device_id_type=MESH,
        )
        copy.start()
        last.append(copy)
    for c in range(2):
        slots = sets[c][1]
        for way in range(2):
            term = product(n - 1, c, way)
            piece(n - 2, c, way, False, True).wait_recv()
            total = slots[way, n - 2].astype(jnp.float32) + term
            out = (gu_out, dn_out)[c]
            if turned:
                out[:, pl.ds(way * half, half)] = total.T
            else:
                out[pl.ds(way * half, half), :] = total
            piece(0, c, way, True).wait_send()
    for copy in last:
        copy.wait()
    total = gain_tp[0]
    for k in range(1, n_tp):
        total = total + gain_tp[k]
    gain_out[...] = total

    def drain(step, carry):
        for c in range(2):
            for way in range(2):
                piece(step, c, way, False).wait_send()
        return carry

    lax.fori_loop(1, n - 1, drain, 0)
    for a in range(2):
        keep(a).wait()
        for away in range(1, n_tp):
            share(a, away).wait()


def reduce(n, n_tp, turned, early_side, cot_side, both, hid, gain, early_all, gu_all, dn_all, late_all):
    rows = gu_all.shape[0] // n
    half = rows // 2
    width = dn_all.shape[1]
    shapes = [(rows, 2 * width), (rows, width)]
    if turned:
        shapes = [shape[::-1] for shape in shapes]
    depth = late_all.shape[1]
    tokens = late_all.shape[0] // n_tp
    vmem = pl.BlockSpec(memory_space=pltpu.VMEM)
    hbm = pl.BlockSpec(memory_space=pl.ANY)
    f32, bf16 = jnp.float32, jnp.bfloat16
    return pl.pallas_call(
        functools.partial(reduce_kernel, n, n_tp, turned),
        out_shape=[
            jax.ShapeDtypeStruct(shapes[0], f32),
            jax.ShapeDtypeStruct(shapes[1], f32),
            jax.ShapeDtypeStruct((n_tp, tokens, depth), bf16),
            jax.ShapeDtypeStruct((n_tp, tokens, depth), bf16),
            jax.ShapeDtypeStruct(gain.shape, f32),
        ],
        in_specs=[vmem] * 6 + [hbm] * 3,
        out_specs=[vmem, vmem, hbm, hbm, vmem],
        scratch_shapes=[
            pltpu.VMEM((2, n - 1, half, 2 * width), bf16),
            pltpu.VMEM((2, n - 1, half, width), bf16),
            pltpu.VMEM((n,) + gain.shape, f32),
            pltpu.VMEM((n_tp,) + gain.shape, f32),
            pltpu.VMEM((2, half, 2 * width), bf16),
            pltpu.VMEM((2, half, width), bf16),
            pltpu.VMEM(gu_all.shape, bf16),
            pltpu.VMEM(dn_all.shape, bf16),
            pltpu.VMEM(late_all.shape, bf16),
            pltpu.VMEM((n_tp, tokens, depth), bf16),
            pltpu.VMEM((n_tp, tokens, depth), bf16),
            pltpu.VMEM(gain.shape, f32),
            pltpu.SemaphoreType.DMA((n - 1, 2, 2)),
            pltpu.SemaphoreType.DMA((n - 1, 2, 2)),
            pltpu.SemaphoreType.DMA((n - 1,)),
            pltpu.SemaphoreType.DMA((n - 1,)),
            pltpu.SemaphoreType.DMA((2, n_tp - 1)),
            pltpu.SemaphoreType.DMA((2, n_tp - 1)),
            pltpu.SemaphoreType.DMA((n_tp - 1,)),
            pltpu.SemaphoreType.DMA((n_tp - 1,)),
            pltpu.SemaphoreType.DMA((3,)),
            pltpu.SemaphoreType.DMA((2,)),
        ],
        compiler_params=pltpu.CompilerParams(
            collective_id=1, has_side_effects=True, vmem_limit_bytes=VMEM_LIMIT
        ),
    )(early_side, cot_side, both, hid, gain, early_all, gu_all, dn_all, late_all)


def per_device(
    n,
    n_tp,
    late_input,
    norm_gain,
    gate_weight,
    up_weight,
    down_weight,
    early_input,
    cotangent,
    gate_sum,
    up_sum,
    down_sum,
    gain_sum,
):
    gain_f = norm_gain.astype(jnp.float32)
    width = gate_weight.shape[1]
    depth = late_input.shape[1]
    turned = gate_weight.shape[0] % 256 == 0
    weights = [gate_weight, up_weight, down_weight]
    if turned:
        weights = [weight.T for weight in weights]
    gain_row = gain_f.reshape(1, depth)
    gu_all, down_all, late_all, early_all, cot_all, d_both, hidden_e = gather(
        n, n_tp, turned, *weights, late_input, early_input, cotangent, gain_row
    )
    sides = (early_all, cot_all) if turned else (early_all.T, cot_all.T)
    gu_grad, down_grad, mix_got, d_got, gain_total = reduce(
        n, n_tp, turned, *sides, d_both, hidden_e, gain_row, early_all, gu_all, down_all, late_all
    )
    if turned:
        gate_grad, up_grad, down_grad = gu_grad[:width].T, gu_grad[width:].T, down_grad.T
    else:
        gate_grad, up_grad = gu_grad[:, :width], gu_grad[:, width:]

    def gathered(got):
        total = got[0].astype(jnp.float32)
        for k in range(1, n_tp):
            total = total + got[k].astype(jnp.float32)
        return total

    values = late_input.astype(jnp.float32)
    values_e = early_input.astype(jnp.float32)
    scale_e = lax.rsqrt(jnp.mean(values_e * values_e, axis=-1, keepdims=True) + epsilon)
    late_out = (values + 0.5 * gathered(mix_got)).astype(jnp.bfloat16)
    scaled_grad = gathered(d_got) * gain_f
    early_grad = (
        cotangent.astype(jnp.float32)
        + scale_e * scaled_grad
        - values_e * scale_e**3 * jnp.mean(values_e * scaled_grad, axis=-1, keepdims=True)
    ).astype(jnp.bfloat16)
    return (
        late_out,
        early_grad,
        gate_sum + gate_grad,
        up_sum + up_grad,
        down_sum + down_grad,
        gain_sum + gain_total.reshape(depth),
    )


def solution(mesh):
    token = P(("fs", "tp"), None)
    weight = P("fs", "tp")
    return jax.shard_map(
        functools.partial(per_device, mesh.shape["fs"], mesh.shape["tp"]),
        mesh=mesh,
        in_specs=(token, P(), weight, weight, weight, token, token, weight, weight, weight, P()),
        out_specs=(token, token, weight, weight, weight, P()),
        check_vma=False,
    )
```
